128 devices in a mesh: sp: 16 (over z, x), tp: 8 (over y, core).
Axes of the slice: x: 4, y: 4, z: 4, core: 2. Of those that a mesh axis runs over, the one named last changes fastest.
Arguments:
- queries: bfloat16 [16384, 1536], P('sp', 'tp'), may hold values from -200 to 200
- key_heads: bfloat16 [16384, 512], P('sp', 'tp'), may hold values from -6 to 6
- projected_value_heads: bfloat16 [16384, 512], P('sp', 'tp'), may hold values from -5 to 5
- sink_logit_table: float32 [24], P('tp'), may hold values from 0 to 4
- out_weight: bfloat16 [1536, 3072], P('tp'), may hold values from -1.5 to 1.5
- residual: bfloat16 [16384, 3072], P('sp', 'tp'), may hold values from -16 to 16
- norm_gain: bfloat16 [3072], P('tp'), may hold values from 0.099609375 to 1.8984375
- up_weight: bfloat16 [3072, 12288], P('sp', 'tp'), may hold values from -0.109375 to 0.109375
- down_weight: bfloat16 [12288, 3072], P('tp', 'sp'), may hold values from -0.0546875 to 0.0546875
Outputs:
- result: bfloat16 [16384, 3072], P('sp', 'tp')
The draws below stay inside these ranges and needn't reach their ends.
All inputs are finite; a program needn't handle non-finite values.
Results may differ from the reference program's by a relative error of at most 0.015.
Values may be sent and summed in bfloat16 or wider, within the bound.
A program may use at most 128 MiB of HBM per device.

```python
import math
import jax
import jax.numpy as jnp
from jax import lax

D = 3072
FF = 12288
QUERY_HEADS = 24
KEY_VALUE_HEADS = 8
HEAD_SIZE = 64
WINDOW_SPAN = 128
SEQUENCE_TOKENS = 16384
N_TP = 8


def inserted_value(key):
    starting_query = jax.random.truncated_normal(jax.random.fold_in(key, 11), -5.0, 5.0, (SEQUENCE_TOKENS, KEY_VALUE_HEADS, QUERY_HEADS // KEY_VALUE_HEADS, HEAD_SIZE), jnp.float32)
    starting_keys = jax.random.truncated_normal(jax.random.fold_in(key, 12), -5.0, 5.0, (SEQUENCE_TOKENS, KEY_VALUE_HEADS, HEAD_SIZE), jnp.float32)
    query_out = starting_query
    keys_out = starting_keys
    return (query_out, keys_out)


def draw_queries(key, part):
    return inserted_value(key)[0].reshape(SEQUENCE_TOKENS, QUERY_HEADS * HEAD_SIZE).astype(jnp.bfloat16)


def draw_key_heads(key, part):
    return inserted_value(key)[1].reshape(SEQUENCE_TOKENS, KEY_VALUE_HEADS * HEAD_SIZE).astype(jnp.bfloat16)


def draw_residual(key, part):
    column = jnp.arange(D).astype(jnp.float32) / (D - 1)
    base = jax.random.truncated_normal(jax.random.fold_in(key, 22), -5.0, 5.0, (SEQUENCE_TOKENS, D), jnp.float32)
    scale = jnp.exp(math.log(3.0) * column)
    return (base * scale[None, :]).astype(jnp.bfloat16)


def shard_levels(rng, dims, split, low, largest):
    def one(position, shards_of):
        steps = jax.random.uniform(jax.random.fold_in(jax.random.fold_in(rng, 6), position), (shards_of,), jnp.float32, low / len(split), largest / len(split))
        return jnp.repeat(jnp.exp(steps), dims[position] // shards_of).reshape((-1,) + (1,) * (len(dims) - position - 1))

    loudness = one(*split[0])
    for cut in split[1:]:
        loudness = loudness * one(*cut)
    return loudness


def noise(stream_key, shape, width, reach, split=(), kind=jnp.bfloat16):
    values = jax.random.normal(stream_key, shape, jnp.float32) * width
    if len(split) > 0:
        values = shard_levels(stream_key, shape, split, -0.22, 0.18) * values
    return jnp.clip(values, min=-reach, max=reach).astype(kind)


def setup_inputs(seed: int = 0) -> dict:
    keys = jax.random.split(jax.random.key(seed), 10)
    queries = draw_queries(jax.random.fold_in(keys[9], 71), 0)
    key_heads = draw_key_heads(jax.random.fold_in(keys[9], 71), 0)
    projected_value_heads = noise(keys[2], (SEQUENCE_TOKENS, KEY_VALUE_HEADS * HEAD_SIZE), 1.0, 5.0, ((0, 16), (1, 8)))
    sink_logit_table = jnp.clip(4.0 * jax.random.uniform(keys[3], (QUERY_HEADS,), jnp.float32) ** shard_levels(keys[3], (QUERY_HEADS,), ((0, 8),), -0.2, 0.2), 0.0, 4.0)
    out_weight = noise(keys[4], (QUERY_HEADS * HEAD_SIZE, D), 0.25, 1.5, ((0, 8),))
    residual = draw_residual(jax.random.fold_in(keys[9], 71), 0)
    norm_gain = jnp.clip(1.0 + 0.18 * jax.random.normal(keys[6], (D,), jnp.float32), 0.099609375, 1.8984375).astype(jnp.bfloat16)
    up_weight = noise(keys[7], (D, FF), D ** -0.5, 0.109375, ((0, 16), (1, 8)))
    down_weight = noise(keys[8], (FF, D), FF ** -0.5, 0.0546875, ((0, 8), (1, 16)))
    return dict(queries=queries, key_heads=key_heads, projected_value_heads=projected_value_heads, sink_logit_table=sink_logit_table, out_weight=out_weight, residual=residual, norm_gain=norm_gain, up_weight=up_weight, down_weight=down_weight)


epsilon = 1e-06

def attend(queries, key_heads, projected_value_heads, sink_logit_table):
    sequence_length = queries.shape[0]
    block_count = sequence_length // WINDOW_SPAN
    group_count = QUERY_HEADS // KEY_VALUE_HEADS
    query_block_list = queries.astype(jnp.float32).reshape(block_count, WINDOW_SPAN, KEY_VALUE_HEADS, group_count, HEAD_SIZE)

    def banded(source_rows):
        padded_rows = jnp.pad(source_rows.astype(jnp.float32).reshape(sequence_length, KEY_VALUE_HEADS, HEAD_SIZE), ((WINDOW_SPAN, 0), (0, 0), (0, 0)))
        padded_rows = padded_rows.reshape(block_count + 1, WINDOW_SPAN, KEY_VALUE_HEADS, HEAD_SIZE)
        return jnp.concatenate([padded_rows[:-1], padded_rows[1:]], axis=1)
    key_band = banded(key_heads)
    value_band = banded(projected_value_heads)
    scores = jnp.einsum('nqkgd,nskd->nkgqs', query_block_list, key_band) * HEAD_SIZE ** (-0.5)
    within = jnp.arange(WINDOW_SPAN)[:, None]
    column = jnp.arange(2 * WINDOW_SPAN)[None, :]
    distance = WINDOW_SPAN + within - column
    valid = (distance >= 0) & (distance < WINDOW_SPAN)
    key_pos = jnp.arange(block_count)[:, None] * WINDOW_SPAN + jnp.arange(2 * WINDOW_SPAN)[None, :] - WINDOW_SPAN
    allowed = valid[None] & (key_pos >= 0)[:, None, :]
    allowed = allowed[:, None, None]
    head_sink_logit = sink_logit_table.astype(jnp.float32).reshape(KEY_VALUE_HEADS, group_count)[None, :, :, None, None]
    masked = jnp.where(allowed, scores, -1e+30)
    ceiling = jnp.maximum(lax.optimization_barrier(jnp.max(masked, axis=-1, keepdims=True)), head_sink_logit)
    powers = jnp.where(allowed, jnp.exp(masked - ceiling), 0.0)
    denom = lax.optimization_barrier(jnp.sum(powers, axis=-1, keepdims=True)) + jnp.exp(head_sink_logit - ceiling)
    probs = (powers / denom).astype(jnp.bfloat16)
    output = jnp.einsum('nkgqs,nskd->nqkgd', probs.astype(jnp.float32), value_band)
    return output.reshape(sequence_length, QUERY_HEADS * HEAD_SIZE).astype(jnp.bfloat16)

def reference(queries, key_heads, projected_value_heads, sink_logit_table, out_weight, residual, norm_gain, up_weight, down_weight):
    attended = attend(queries, key_heads, projected_value_heads, sink_logit_table)
    head_cols = QUERY_HEADS * HEAD_SIZE // N_TP
    mixed = jnp.zeros(residual.shape, jnp.float32)
    for group in range(N_TP):
        part = jnp.dot(attended[:, group * head_cols:(group + 1) * head_cols], out_weight[group * head_cols:(group + 1) * head_cols], preferred_element_type=jnp.float32)
        part = lax.optimization_barrier(part.astype(jnp.bfloat16))
        mixed = mixed + part.astype(jnp.float32)
    stream = lax.optimization_barrier((residual.astype(jnp.float32) + mixed).astype(jnp.bfloat16)).astype(jnp.float32)
    mean_square = lax.optimization_barrier(jnp.mean(stream * stream, axis=-1, keepdims=True)) + epsilon
    normed = (stream * lax.rsqrt(mean_square) * norm_gain.astype(jnp.float32)).astype(jnp.bfloat16)
    unit_cols = FF // N_TP
    branch_sum = jnp.zeros(residual.shape, jnp.float32)
    for group in range(N_TP):
        hidden_pre = jnp.dot(normed, up_weight[:, group * unit_cols:(group + 1) * unit_cols], preferred_element_type=jnp.float32)
        activated = jnp.square(jax.nn.relu(hidden_pre)).astype(jnp.bfloat16)
        branch = jnp.dot(activated, down_weight[group * unit_cols:(group + 1) * unit_cols], preferred_element_type=jnp.float32)
        branch = lax.optimization_barrier(branch.astype(jnp.bfloat16))
        branch_sum = branch_sum + branch.astype(jnp.float32)
    return (stream + branch_sum).astype(jnp.bfloat16)
```

```python
import functools

import jax
import jax.numpy as jnp
from jax import lax
from jax.experimental import pallas as pl
from jax.experimental.pallas import tpu as pltpu
from jax.sharding import PartitionSpec as P

D = 3072
HEAD_SIZE = 64
WINDOW = 128
EPSILON = 1e-06

ROWS = 1024
FEATURES = 384
HEADS = 192
SHARD = 192
HALF = 96
QUARTER = 48
HIDDEN = 1536
TILE = 256

MESH = pl.DeviceIdType.MESH
BF16 = jnp.bfloat16
F32 = jnp.float32


def dot(a, b, dims):
    return lax.dot_general(a, b, (dims, ((), ())), preferred_element_type=F32)


def kernel(
    queries, keys, values, sink, out_weight, residual, gain, up, down,
    result,
    up_all, down_all, x_all, att_all, w_all, hidden, act, mixed, stream, res_v,
    q_v, k_v, v_v, halo_k, halo_v, partials, paired, chained, final, squares, inverse, out_v,
    local_sem, w_send, w_recv, halo_send, halo_recv, g_send, g_recv,
    att_send, att_recv, x_send, x_recv, sq_send, sq_recv,
    pair_send, pair_recv, chain_send, chain_recv, final_send, final_recv,
):
    s, t = lax.axis_index("sp"), lax.axis_index("tp")
    z, x = s // 4, s % 4
    y, c = t // 2, t % 2

    def ring(position, by):
        return (position + by + 4) % 4

    def device(zz, xx, yy, cc):
        return (zz * 4 + xx, yy * 2 + cc)

    partner = (s, y * 2 + (1 - c))
    y_next = {1: (s, ring(y, 1) * 2 + c), -1: (s, ring(y, -1) * 2 + c)}
    DIRS = ((0, 1), (1, -1))

    def remote(src, dst, send, recv, target):
        return pltpu.make_async_remote_copy(
            src_ref=src, dst_ref=dst, send_sem=send, recv_sem=recv,
            device_id=target, device_id_type=MESH,
        )

    pending = []

    def start(copy):
        copy.start()
        pending.append(copy)

    barrier = pltpu.get_barrier_semaphore()
    greeted = [
        device(z, ring(x, 1), y, c), device(z, ring(x, -1), y, c),
        device(ring(z, 1), x, y, c), device(ring(z, -1), x, y, c),
        ((s + 1) % 16, t), ((s + 15) % 16, t),
    ] + [(s, (t + k) % 8) for k in range(1, 8)]
    for other in greeted:
        pl.semaphore_signal(barrier, inc=1, device_id=other, device_id_type=MESH)
    locals_ = [
        pltpu.make_async_copy(src, dst, local_sem.at[i])
        for i, (src, dst) in enumerate([
            (queries, q_v), (keys, k_v), (values, v_v), (residual, res_v),
            (up, up_all.at[pl.ds(pl.multiple_of(s * SHARD, SHARD), SHARD)]),
            (down, down_all.at[pl.ds(pl.multiple_of(s * SHARD, SHARD), SHARD)]),
            (out_weight.at[:, pl.ds(pl.multiple_of(t * FEATURES, 128), FEATURES)],
             w_all.at[pl.ds(pl.multiple_of(t * HEADS, HEADS), HEADS)]),
        ])
    ]
    for copy in locals_:
        copy.start()
    pl.semaphore_wait(barrier, len(greeted))

    STEPS = (0, -1, 1, 2)

    class Gather:
        def __init__(self, own, buf, base):
            self.own, self.buf, self.base = own, buf, base

        def spot(self, half, sec, prim, low, count):
            zz, xx = (sec, prim) if half == 0 else (prim, sec)
            row = (zz * 4 + xx) * SHARD + half * HALF + low
            return self.buf.at[pl.ds(pl.multiple_of(row, 16), count)]

        def copy(self, half, index, src, dst, target):
            k = self.base + half * 20 + index
            return remote(src, dst, g_send.at[k], g_recv.at[k], target)

        def at(self, half):
            return (z, x) if half == 0 else (x, z)

        def towards(self, half, primary, by):
            if primary == (half == 0):
                return device(z, ring(x, by), y, c)
            return device(ring(z, by), x, y, c)

        def first(self):
            for half in (0, 1):
                sec, prim = self.at(half)
                src = self.own.at[pl.ds(half * HALF, HALF)]
                dst = self.spot(half, sec, prim, 0, HALF)
                for d, by in DIRS:
                    start(self.copy(half, d, src, dst, self.towards(half, True, by)))
            for half in (0, 1):
                sec, prim = self.at(half)
                src = self.own.at[pl.ds(half * HALF, HALF)]
                dst = self.spot(half, sec, prim, 0, HALF)
                for d, by in DIRS:
                    start(self.copy(half, 4 + d, src, dst, self.towards(half, False, by)))

        def wait(self, half, index, sec, prim, low, count):
            ref = self.spot(half, sec, prim, low, count)
            self.copy(half, index, ref, ref, partner).wait_recv()

        def second(self):
            for half in (0, 1):
                sec, prim = self.at(half)
                for d, by in DIRS:
                    origin = ring(prim, -by)
                    self.wait(half, d, sec, origin, 0, HALF)
                    piece = self.spot(half, sec, origin, d * QUARTER, QUARTER)
                    start(self.copy(half, 2 + d, piece, piece, self.towards(half, True, by)))
            for half in (0, 1):
                for j in (1, 2):
                    self.spread(half, j)

        def spread(self, half, j):
            sec, prim = self.at(half)
            piece = self.spot(half, sec, ring(prim, STEPS[j]), 0, HALF)
            for d, by in DIRS:
                start(self.copy(half, 4 + 2 * j + d, piece, piece, self.towards(half, False, by)))

        def third(self):
            for half in (0, 1):
                sec, prim = self.at(half)
                for d, by in DIRS:
                    self.wait(half, 2 + d, sec, ring(prim, 2), d * QUARTER, QUARTER)
                self.spread(half, 3)

        def forward(self, j):
            for half in (0, 1):
                sec, prim = self.at(half)
                origin = ring(prim, STEPS[j])
                for d, by in DIRS:
                    self.wait(half, 4 + 2 * j + d, ring(sec, -by), origin, 0, HALF)
                    piece = self.spot(half, ring(sec, -by), origin, d * QUARTER, QUARTER)
                    start(self.copy(half, 12 + 2 * j + d, piece, piece, self.towards(half, False, by)))

        def last(self, j):
            for half in (0, 1):
                sec, prim = self.at(half)
                origin = ring(prim, STEPS[j])
                for d, by in DIRS:
                    self.wait(half, 12 + 2 * j + d, ring(sec, 2), origin, d * QUARTER, QUARTER)

    up_gather = Gather(up, up_all, 0)
    down_gather = Gather(down, down_all, 40)
    up_gather.first()

    after = ((s + 1) % 16, t)
    tail = pl.ds(ROWS - WINDOW, WINDOW)
    halo_copies = [
        remote(keys.at[:, tail], halo_k, halo_send.at[0], halo_recv.at[0], after),
        remote(values.at[:, tail], halo_v, halo_send.at[1], halo_recv.at[1], after),
    ]
    for copy in halo_copies:
        start(copy)
    w_mine = w_all.at[pl.ds(pl.multiple_of(t * HEADS, HEADS), HEADS)]
    w_copies = []
    for k in range(1, 8):
        owner = (t + k) % 8
        copy = remote(
            out_weight.at[:, pl.ds(pl.multiple_of(owner * FEATURES, 128), FEATURES)],
            w_mine, w_send.at[k - 1], w_recv.at[k - 1], (s, owner),
        )
        start(copy)
        w_copies.append(copy)

    sinks = jnp.concatenate([jnp.full((1, WINDOW), sink[g], F32) for g in range(3)], axis=1)
    key_at = lax.broadcasted_iota(jnp.int32, (2 * WINDOW, 3 * WINDOW), 0)
    query_at = lax.broadcasted_iota(jnp.int32, (2 * WINDOW, 3 * WINDOW), 1) % WINDOW
    mine_row = t * HEADS

    def attend(n, key_band, value_band, allowed):
        lanes = pl.ds(pl.multiple_of(n * WINDOW, WINDOW), WINDOW)
        q = jnp.concatenate([q_v[pl.ds(g * HEAD_SIZE, HEAD_SIZE), lanes] for g in range(3)], axis=1)
        scores = dot(key_band, q, ((0,), (0,))) * HEAD_SIZE**-0.5
        masked = jnp.where(allowed, scores, -1e30)
        top = jnp.maximum(jnp.max(masked, axis=0, keepdims=True), sinks)
        powers = jnp.where(allowed, jnp.exp(masked - top), 0.0)
        denom = jnp.sum(powers, axis=0, keepdims=True) + jnp.exp(sinks - top)
        probs = (powers * (1.0 / denom)).astype(BF16)
        output = dot(value_band, probs, ((1,), (0,))).astype(BF16)
        for g in range(3):
            rows = pl.ds(pl.multiple_of(mine_row + g * HEAD_SIZE, HEAD_SIZE), HEAD_SIZE)
            att_all[rows, lanes] = output[:, g * WINDOW : (g + 1) * WINDOW]

    near = (key_at > query_at) & (key_at <= query_at + WINDOW)
    for copy in locals_[:3]:
        copy.wait()

    @pl.loop(1, 8)
    def _(n):
        band = pl.ds(pl.multiple_of((n - 1) * WINDOW, WINDOW), 2 * WINDOW)
        attend(n, k_v[:, band], v_v[:, band], near)

    for copy in halo_copies:
        copy.wait_recv()
    first_key = jnp.where(s == 0, WINDOW, 0)
    attend(
        0,
        jnp.concatenate([halo_k[...], k_v[:, 0:WINDOW]], axis=1),
        jnp.concatenate([halo_v[...], v_v[:, 0:WINDOW]], axis=1),
        near & (key_at >= first_key),
    )

    def att_rows(yy, cc, low=0, count=HEADS):
        row = (yy * 2 + cc) * HEADS + low
        return att_all.at[pl.ds(pl.multiple_of(row, 32), count)]

    def att_copy(index, ref, target):
        return remote(ref, ref, att_send.at[index], att_recv.at[index], target)

    def att_arrived(index, ref):
        att_copy(index, ref, partner).wait_recv()

    for d, by in DIRS:
        start(att_copy(d, att_rows(y, c), y_next[by]))
    start(att_copy(4, att_rows(y, c), partner))
    up_gather.second()

    for i, copy in enumerate(locals_[3:]):
        copy.wait()
    for copy in w_copies:
        copy.wait_recv()

    def mix(yy, first):
        rows = pl.ds(pl.multiple_of(yy * 2 * HEADS, 2 * HEADS), 2 * HEADS)

        @pl.loop(0, ROWS // TILE)
        def _(i):
            tokens = pl.ds(pl.multiple_of(i * TILE, TILE), TILE)
            part = dot(att_all[rows, tokens], w_all[rows, :], ((0,), (0,)))
            mixed[tokens, :] = part if first else mixed[tokens, :] + part

    att_arrived(4, att_rows(y, 1 - c))
    mix(y, True)
    for d, by in DIRS:
        att_arrived(d, att_rows(ring(y, -by), c))
        start(att_copy(2 + d, att_rows(ring(y, -by), c, d * HALF, HALF), y_next[by]))
        start(att_copy(5 + d, att_rows(ring(y, -by), c), partner))
    up_gather.third()
    for d, by in DIRS:
        att_arrived(5 + d, att_rows(ring(y, -by), 1 - c))
        mix(ring(y, -by), False)
    for d, by in DIRS:
        att_arrived(2 + d, att_rows(ring(y, 2), c, d * HALF, HALF))
    start(att_copy(7, att_rows(ring(y, 2), c), partner))
    att_arrived(7, att_rows(ring(y, 2), 1 - c))
    mix(ring(y, 2), False)

    lanes_of = lambda cc: pl.ds(pl.multiple_of(cc * FEATURES, 128), FEATURES)

    def x_block(yy, cc, low=0, count=ROWS):
        return x_all.at[pl.ds(pl.multiple_of(yy * ROWS + low, 512), count), lanes_of(cc)]

    gains = gain[...].astype(F32)
    ones = jnp.ones((8, FEATURES), BF16)
    sq_rows = pl.ds(pl.multiple_of(t * 8, 8), 8)

    @pl.loop(0, ROWS // TILE)
    def _(i):
        tokens = pl.ds(pl.multiple_of(i * TILE, TILE), TILE)
        here = (res_v[tokens, :].astype(F32) + mixed[tokens, :]).astype(BF16)
        stream[tokens, :] = here
        wide = here.astype(F32)
        x_all[pl.ds(pl.multiple_of(y * ROWS + i * TILE, TILE), TILE), lanes_of(c)] = (wide * gains).astype(BF16)
        sq = wide * wide
        high = sq.astype(BF16)
        low = (sq - high.astype(F32)).astype(BF16)
        squares[sq_rows, tokens] = dot(ones, high, ((1,), (1,))) + dot(ones, low, ((1,), (1,)))

    def x_copy(index, ref, target):
        return remote(ref, ref, x_send.at[index], x_recv.at[index], target)

    def x_arrived(index, ref):
        x_copy(index, ref, partner).wait_recv()

    for part in (0, 1):
        for d, by in DIRS:
            start(x_copy(2 * part + d, x_block(y, c, part * 512, 512), y_next[by]))
    start(x_copy(6, x_block(y, c), partner))
    sq_copies = []
    for k in range(1, 8):
        ref = squares.at[sq_rows]
        copy = remote(ref, ref, sq_send.at[k - 1], sq_recv.at[k - 1], (s, (t + k) % 8))
        start(copy)
        sq_copies.append(copy)

    up_gather.forward(0)
    up_gather.forward(1)
    up_gather.forward(2)
    x_arrived(0, x_block(ring(y, -1), c, 0, 512))
    start(x_copy(4, x_block(ring(y, -1), c, 0, 512), y_next[1]))
    x_arrived(1, x_block(ring(y, 1), c, 0, 512))
    up_gather.forward(3)
    down_gather.first()
    x_arrived(3, x_block(ring(y, 1), c, 512, 512))
    start(x_copy(5, x_block(ring(y, 1), c, 512, 512), y_next[-1]))
    x_arrived(2, x_block(ring(y, -1), c, 512, 512))
    start(x_copy(7, x_block(ring(y, -1), c), partner))
    start(x_copy(8, x_block(ring(y, 1), c), partner))

    def hide(yy, first, last):
        @pl.loop(0, ROWS // TILE)
        def _(i):
            tokens = pl.ds(pl.multiple_of(i * TILE, TILE), TILE)
            block = x_all[pl.ds(pl.multiple_of(yy * ROWS + i * TILE, TILE), TILE), :]
            for n in range(3):
                cols = pl.ds(n * 512, 512)
                part = dot(block, up_all[pl.ds(pl.multiple_of(yy * 768, 768), 768), cols], ((1,), (0,)))
                if not first:
                    part = part + hidden[tokens, cols]
                if last:
                    act[tokens, cols] = jnp.square(jnp.maximum(part, 0.0)).astype(BF16)
                else:
                    hidden[tokens, cols] = part

    for j in range(4):
        up_gather.last(j)
    x_arrived(6, x_block(y, 1 - c))
    hide(y, True, False)
    for d, by in DIRS:
        x_arrived(7 + d, x_block(ring(y, -by), 1 - c))
        hide(ring(y, -by), False, False)
    x_arrived(4, x_block(ring(y, 2), c, 0, 512))
    x_arrived(5, x_block(ring(y, 2), c, 512, 512))
    start(x_copy(9, x_block(ring(y, 2), c), partner))
    down_gather.second()
    x_arrived(9, x_block(ring(y, 2), 1 - c))
    hide(ring(y, 2), False, True)

    for copy in sq_copies:
        copy.wait_recv()
    total = jnp.zeros((1, ROWS), F32)
    for k in range(8):
        total = total + squares[pl.ds(8 * k, 1), :]
    factor = 1.0 / (total * (1.0 / D) + EPSILON)
    inverse[...] = jnp.transpose(jnp.broadcast_to(factor, (128, ROWS)))

    own_pair = x // 2
    BLOCKS = ((0, 0), (0, 1), (0, 2), (1, 0), (0, 3), (1, 1), (1, 2), (1, 3))
    SHIFT = (0, 1, -1, 2)

    def slot(kind, j):
        return pl.ds(pl.multiple_of((kind * 4 + j) * ROWS, ROWS), ROWS)

    def pair_slot(j):
        return pl.ds(pl.multiple_of(j * ROWS, ROWS), ROWS)

    def facts(kind, j):
        pair = own_pair if kind == 0 else 1 - own_pair
        owner = ring(z, SHIFT[j])
        return pair, owner, c == pair, (y - owner + 4) % 4

    def pair_copy(kind, j):
        return remote(
            partials.at[slot(kind, j)], paired.at[pair_slot(j)],
            pair_send.at[j], pair_recv.at[j], partner,
        )

    def compute(kind, j):
        pair, owner, combines, _ = facts(kind, j)
        weight = pl.ds(pl.multiple_of((owner * 4 + pair * 2) * SHARD, 2 * SHARD), 2 * SHARD)

        @pl.loop(0, ROWS // TILE)
        def _(i):
            tokens = pl.ds(pl.multiple_of(i * TILE, TILE), TILE)
            part = dot(act[tokens, :], down_all[weight, :], ((1,), (1,)))
            rows = pl.ds(pl.multiple_of((kind * 4 + j) * ROWS + i * TILE, TILE), TILE)
            partials[rows, :] = part.astype(BF16)

        @pl.when(jnp.logical_not(combines))
        def _():
            pair_copy(kind, j).start()

    def add_rows(kind, j, extra, low, count):
        @pl.loop(0, count // 128)
        def _(i):
            rows = pl.ds(pl.multiple_of((kind * 4 + j) * ROWS + low + i * 128, 128), 128)
            there = pl.ds(pl.multiple_of(j * ROWS + low + i * 128, 128), 128)
            total = partials[rows, :].astype(F32) + paired[there, :].astype(F32)
            if extra is not None:
                total = total + chained[pl.ds(pl.multiple_of(extra * 512 + i * 128, 128), 128), :].astype(F32)
            partials[rows, :] = total.astype(BF16)

    def chain_copy(d, src, target):
        return remote(src, chained.at[pl.ds(d * 512, 512)], chain_send.at[d], chain_recv.at[d], target)

    def final_copy(d, src, target):
        return remote(src, final.at[pl.ds(d * ROWS, ROWS)], final_send.at[d], final_recv.at[d], target)

    def half_of(kind, j, d):
        return partials.at[pl.ds(pl.multiple_of((kind * 4 + j) * ROWS + d * 512, 512), 512)]

    def combine(kind, j):
        _, _, combines, d = facts(kind, j)

        @pl.when(combines & (d == 2))
        def _():
            pair_copy(kind, j).wait_recv()
            add_rows(kind, j, None, 0, ROWS)
            for k, by in DIRS:
                chain_copy(k, half_of(kind, j, k), y_next[by]).start()

    def relay(kind, j):
        _, _, combines, d = facts(kind, j)
        for k, by in DIRS:
            @pl.when(combines & (d == (3 if k == 0 else 1)))
            def _():
                pair_copy(kind, j).wait_recv()
                add_rows(kind, j, None, (1 - k) * 512, 512)
                chain_copy(k, half_of(kind, j, k), y_next[by]).wait_recv()
                add_rows(kind, j, k, k * 512, 512)
                final_copy(k, partials.at[slot(kind, j)], y_next[by]).start()

    down_gather.forward(0)
    compute(*BLOCKS[0])
    down_gather.third()
    combine(*BLOCKS[0])
    down_gather.forward(1)
    down_gather.forward(2)
    compute(*BLOCKS[1])
    combine(*BLOCKS[1])
    relay(*BLOCKS[0])
    compute(*BLOCKS[2])
    combine(*BLOCKS[2])
    relay(*BLOCKS[1])
    down_gather.forward(3)
    down_gather.last(0)
    compute(*BLOCKS[3])
    relay(*BLOCKS[2])
    combine(*BLOCKS[3])
    down_gather.last(1)
    down_gather.last(2)
    compute(*BLOCKS[4])
    compute(*BLOCKS[5])
    combine(*BLOCKS[4])
    relay(*BLOCKS[3])
    compute(*BLOCKS[6])
    combine(*BLOCKS[5])
    relay(*BLOCKS[4])
    down_gather.last(3)
    compute(*BLOCKS[7])
    combine(*BLOCKS[6])
    relay(*BLOCKS[5])
    combine(*BLOCKS[7])
    relay(*BLOCKS[6])
    relay(*BLOCKS[7])

    kind = jnp.where(c == own_pair, 0, 1)
    away = (y - z + 4) % 4
    j = jnp.where(away == 3, 2, jnp.where(away == 2, 3, away))
    pair_copy(kind, j).wait_recv()
    for k, by in DIRS:
        final_copy(k, partials.at[slot(kind, j)], y_next[by]).wait_recv()

    @pl.loop(0, ROWS // 128)
    def _(i):
        tokens = pl.ds(pl.multiple_of(i * 128, 128), 128)

        def rows(base):
            return pl.ds(pl.multiple_of(base * ROWS + i * 128, 128), 128)

        total = partials[rows(kind * 4 + j), :].astype(F32) + paired[rows(j), :].astype(F32)
        total = total + (final[rows(0), :].astype(F32) + final[rows(1), :].astype(F32))
        scale = inverse[tokens, :]
        scale = jnp.concatenate([scale, scale, scale], axis=1)
        out_v[tokens, :] = (stream[tokens, :].astype(F32) + scale * total).astype(BF16)

    store = pltpu.make_async_copy(out_v, result, local_sem.at[7])
    store.start()
    for copy in pending:
        copy.wait_send()
    other = 1 - kind
    for k in range(4):
        pair_copy(other, k).wait_send()
    for k, by in DIRS:
        chain_copy(k, half_of(kind, j, k), y_next[by]).wait_send()
        final_copy(k, partials.at[slot(kind, j)], y_next[by]).wait_send()
    store.wait()


def body(
    queries, key_heads, projected_value_heads, sink_logit_table, out_weight,
    residual, norm_gain, up_weight, down_weight,
):
    hbm = pl.BlockSpec(memory_space=pl.ANY)
    dma = pltpu.SemaphoreType.DMA
    return pl.pallas_call(
        kernel,
        out_shape=jax.ShapeDtypeStruct((ROWS, FEATURES), BF16),
        in_specs=[hbm, hbm, hbm, pl.BlockSpec(memory_space=pltpu.SMEM), hbm, hbm,
                  pl.BlockSpec(memory_space=pltpu.VMEM), hbm, hbm],
        out_specs=hbm,
        scratch_shapes=[
            pltpu.VMEM((D, HIDDEN), BF16),
            pltpu.VMEM((D, HIDDEN), BF16),
            pltpu.VMEM((4 * ROWS, 2 * FEATURES), BF16),
            pltpu.VMEM((8 * HEADS, ROWS), BF16),
            pltpu.VMEM((8 * HEADS, FEATURES), BF16),
            pltpu.VMEM((ROWS, HIDDEN), F32),
            pltpu.VMEM((ROWS, HIDDEN), BF16),
            pltpu.VMEM((ROWS, FEATURES), F32),
            pltpu.VMEM((ROWS, FEATURES), BF16),
            pltpu.VMEM((ROWS, FEATURES), BF16),
            pltpu.VMEM((HEADS, ROWS), BF16),
            pltpu.VMEM((HEAD_SIZE, ROWS), BF16),
            pltpu.VMEM((HEAD_SIZE, ROWS), BF16),
            pltpu.VMEM((HEAD_SIZE, WINDOW), BF16),
            pltpu.VMEM((HEAD_SIZE, WINDOW), BF16),
            pltpu.VMEM((8 * ROWS, FEATURES), BF16),
            pltpu.VMEM((4 * ROWS, FEATURES), BF16),
            pltpu.VMEM((2 * 512, FEATURES), BF16),
            pltpu.VMEM((2 * ROWS, FEATURES), BF16),
            pltpu.VMEM((64, ROWS), F32),
            pltpu.VMEM((ROWS, 128), F32),
            pltpu.VMEM((ROWS, FEATURES), BF16),
            dma((8,)), dma((7,)), dma((7,)), dma((2,)), dma((2,)), dma((80,)), dma((80,)),
            dma((8,)), dma((8,)), dma((10,)), dma((10,)), dma((7,)), dma((7,)),
            dma((4,)), dma((4,)), dma((2,)), dma((2,)), dma((2,)), dma((2,)),
        ],
        compiler_params=pltpu.CompilerParams(
            collective_id=0, has_side_effects=True, vmem_limit_bytes=67043328
        ),
    )(
        queries.T, key_heads.T, projected_value_heads.T, sink_logit_table, out_weight,
        residual, norm_gain.reshape(1, FEATURES), up_weight, down_weight.T,
    )


def solution(mesh):
    return jax.shard_map(
        body,
        mesh=mesh,
        in_specs=(
            P("sp", "tp"), P("sp", "tp"), P("sp", "tp"), P("tp"), P("tp", None),
            P("sp", "tp"), P("tp"), P("sp", "tp"), P("tp", "sp"),
        ),
        out_specs=P("sp", "tp"),
        check_vma=False,
    )
```

```python
import functools

import jax
import jax.numpy as jnp
from jax import lax
from jax.experimental import pallas as pl
from jax.experimental.pallas import tpu as pltpu
from jax.sharding import PartitionSpec as P

D = 3072
HEAD_SIZE = 64
WINDOW = 128
EPSILON = 1e-06

ROWS = 1024
FEATURES = 384
HEADS = 192
SHARD = 192
HALF = 96
QUARTER = 48
HIDDEN = 1536
TILE = 256

MESH = pl.DeviceIdType.MESH
BF16 = jnp.bfloat16
F32 = jnp.float32


def dot(a, b, dims):
    return lax.dot_general(a, b, (dims, ((), ())), preferred_element_type=F32)


def kernel(
    queries, keys, values, sink, out_weight, residual, gain, up, down,
    result,
    up_all, down_all, x_all, att_all, w_all, w_pass, hidden, act_t, mixed, stream, res_v,
    q_v, k_v, v_v, halo_k, halo_v, partials, paired, chained, final, squares, out_v,
    local_sem, w_send, w_recv, halo_send, halo_recv, g_send, g_recv,
    att_send, att_recv, x_send, x_recv, sq_send, sq_recv,
    pair_send, pair_recv, chain_send, chain_recv,
):
    s, t = lax.axis_index("sp"), lax.axis_index("tp")
    z, x = s // 4, s % 4
    y, c = t // 2, t % 2

    def ring(position, by):
        return (position + by + 4) % 4

    def device(zz, xx, yy, cc):
        return (zz * 4 + xx, yy * 2 + cc)

    partner = (s, y * 2 + (1 - c))
    y_next = {1: (s, ring(y, 1) * 2 + c), -1: (s, ring(y, -1) * 2 + c)}
    DIRS = ((0, 1), (1, -1))

    def remote(src, dst, send, recv, target):
        return pltpu.make_async_remote_copy(
            src_ref=src, dst_ref=dst, send_sem=send, recv_sem=recv,
            device_id=target, device_id_type=MESH,
        )

    pending = []

    def start(copy):
        copy.start()
        pending.append(copy)

    barrier = pltpu.get_barrier_semaphore()
    greeted = [
        device(z, ring(x, 1), y, c), device(z, ring(x, -1), y, c),
        device(ring(z, 1), x, y, c), device(ring(z, -1), x, y, c),
        ((s + 1) % 16, t), ((s + 15) % 16, t),
    ] + [(s, (t + k) % 8) for k in range(1, 8)]
    for other in greeted:
        pl.semaphore_signal(barrier, inc=1, device_id=other, device_id_type=MESH)
    locals_ = [
        pltpu.make_async_copy(src, dst, local_sem.at[i])
        for i, (src, dst) in enumerate([
            (queries, q_v), (keys, k_v), (values, v_v), (residual, res_v),
            (up, up_all.at[pl.ds(pl.multiple_of(s * SHARD, SHARD), SHARD)]),
            (down, down_all.at[pl.ds(pl.multiple_of(s * SHARD, SHARD), SHARD)]),
            (out_weight.at[:, pl.ds(pl.multiple_of(t * FEATURES, 128), FEATURES)],
             w_all.at[pl.ds(pl.multiple_of(t * HEADS, HEADS), HEADS)]),
        ])
    ]
    for copy in locals_:
        copy.start()
    pl.semaphore_wait(barrier, len(greeted))

    STEPS = (0, -1, 1, 2)

    class Gather:
        def __init__(self, own, buf, base):
            self.own, self.buf, self.base = own, buf, base

        def spot(self, half, sec, prim, low, count):
            zz, xx = (sec, prim) if half == 0 else (prim, sec)
            row = (zz * 4 + xx) * SHARD + half * HALF + low
            return self.buf.at[pl.ds(pl.multiple_of(row, 16), count)]

        def copy(self, half, index, src, dst, target):
            k = self.base + half * 20 + index
            return remote(src, dst, g_send.at[k], g_recv.at[k], target)

        def at(self, half):
            return (z, x) if half == 0 else (x, z)

        def towards(self, half, primary, by):
            if primary == (half == 0):
                return device(z, ring(x, by), y, c)
            return device(ring(z, by), x, y, c)

        def first(self):
            for half in (0, 1):
                sec, prim = self.at(half)
                src = self.own.at[pl.ds(half * HALF, HALF)]
                dst = self.spot(half, sec, prim, 0, HALF)
                for d, by in DIRS:
                    start(self.copy(half, d, src, dst, self.towards(half, True, by)))
            for half in (0, 1):
                sec, prim = self.at(half)
                src = self.own.at[pl.ds(half * HALF, HALF)]
                dst = self.spot(half, sec, prim, 0, HALF)
                for d, by in DIRS:
                    start(self.copy(half, 4 + d, src, dst, self.towards(half, False, by)))

        def wait(self, half, index, sec, prim, low, count):
            ref = self.spot(half, sec, prim, low, count)
            self.copy(half, index, ref, ref, partner).wait_recv()

        def second(self):
            for half in (0, 1):
                sec, prim = self.at(half)
                for d, by in DIRS:
                    origin = ring(prim, -by)
                    self.wait(half, d, sec, origin, 0, HALF)
                    piece = self.spot(half, sec, origin, d * QUARTER, QUARTER)
                    start(self.copy(half, 2 + d, piece, piece, self.towards(half, True, by)))
            for half in (0, 1):
                for j in (1, 2):
                    self.spread(half, j)

        def spread(self, half, j):
            sec, prim = self.at(half)
            piece = self.spot(half, sec, ring(prim, STEPS[j]), 0, HALF)
            for d, by in DIRS:
                start(self.copy(half, 4 + 2 * j + d, piece, piece, self.towards(half, False, by)))

        def third(self):
            for half in (0, 1):
                sec, prim = self.at(half)
                for d, by in DIRS:
                    self.wait(half, 2 + d, sec, ring(prim, 2), d * QUARTER, QUARTER)
                self.spread(half, 3)

        def forward(self, j):
            for half in (0, 1):
                sec, prim = self.at(half)
                origin = ring(prim, STEPS[j])
                for d, by in DIRS:
                    self.wait(half, 4 + 2 * j + d, ring(sec, -by), origin, 0, HALF)
                    piece = self.spot(half, ring(sec, -by), origin, d * QUARTER, QUARTER)
                    start(self.copy(half, 12 + 2 * j + d, piece, piece, self.towards(half, False, by)))

        def last(self, j):
            for half in (0, 1):
                sec, prim = self.at(half)
                origin = ring(prim, STEPS[j])
                for d, by in DIRS:
                    self.wait(half, 12 + 2 * j + d, ring(sec, 2), origin, d * QUARTER, QUARTER)

    up_gather = Gather(up, up_all, 0)
    down_gather = Gather(down, down_all, 40)
    after = ((s + 1) % 16, t)
    tail = pl.ds(ROWS - WINDOW, WINDOW)
    halo_copies = [
        remote(keys.at[:, tail], halo_k, halo_send.at[0], halo_recv.at[0], after),
        remote(values.at[:, tail], halo_v, halo_send.at[1], halo_recv.at[1], after),
    ]
    for copy in halo_copies:
        start(copy)
    up_gather.first()

    def w_cols(yy, cc=0, count=FEATURES):
        return pl.ds(pl.multiple_of((yy * 2 + cc) * FEATURES, 128), count)

    def w_rows(yy, cc, low=0, count=HEADS):
        return w_all.at[pl.ds(pl.multiple_of((yy * 2 + cc) * HEADS + low, 32), count)]

    def w_relay(k, by):
        src = out_weight.at[pl.ds(k * HALF, HALF), w_cols(ring(y, 2), 0, 2 * FEATURES)]
        return remote(src, w_pass.at[k], w_send.at[5 + k], w_recv.at[5 + k], y_next[by])

    for k, by in DIRS:
        start(w_relay(k, by))
    start(remote(out_weight.at[:, w_cols(y, 1 - c)], w_rows(y, c), w_send.at[0], w_recv.at[0], partner))
    for k, by in DIRS:
        for cc in (0, 1):
            start(remote(
                out_weight.at[:, w_cols(ring(y, by), cc)], w_rows(y, c),
                w_send.at[1 + 2 * k + cc], w_recv.at[1 + 2 * k + c], (s, ring(y, by) * 2 + cc),
            ))

    def w_arrived(index, ref):
        remote(ref, ref, w_send.at[index], w_recv.at[index], partner).wait_recv()

    def w_pass_on():
        for k, by in DIRS:
            w_relay(k, by).wait_recv()
            for cc in (0, 1):
                start(remote(
                    w_pass.at[k, :, pl.ds(cc * FEATURES, FEATURES)], w_rows(ring(y, -by), c, k * HALF, HALF),
                    w_send.at[7 + 2 * k + cc], w_recv.at[7 + 2 * k + c], (s, ring(y, by) * 2 + cc),
                ))

    sinks = jnp.concatenate([jnp.full((1, WINDOW), sink[g], F32) for g in range(3)], axis=1)
    key_at = lax.broadcasted_iota(jnp.int32, (2 * WINDOW, 3 * WINDOW), 0)
    query_at = lax.broadcasted_iota(jnp.int32, (2 * WINDOW, 3 * WINDOW), 1) % WINDOW
    mine_row = t * HEADS

    def attend(n, key_band, value_band, allowed):
        lanes = pl.ds(pl.multiple_of(n * WINDOW, WINDOW), WINDOW)
        q = jnp.concatenate([q_v[pl.ds(g * HEAD_SIZE, HEAD_SIZE), lanes] for g in range(3)], axis=1)
        scores = dot(key_band, q, ((0,), (0,))) * HEAD_SIZE**-0.5
        masked = jnp.where(allowed, scores, -1e30)
        top = jnp.maximum(jnp.max(masked, axis=0, keepdims=True), sinks)
        powers = jnp.where(allowed, jnp.exp(masked - top), 0.0)
        denom = jnp.sum(powers, axis=0, keepdims=True) + jnp.exp(sinks - top)
        probs = (powers * (1.0 / denom)).astype(BF16)
        output = dot(value_band, probs, ((1,), (0,))).astype(BF16)
        for g in range(3):
            rows = pl.ds(pl.multiple_of(mine_row + g * HEAD_SIZE, HEAD_SIZE), HEAD_SIZE)
            att_all[rows, lanes] = output[:, g * WINDOW : (g + 1) * WINDOW]

    near = (key_at > query_at) & (key_at <= query_at + WINDOW)
    for copy in locals_[:3]:
        copy.wait()

    @pl.loop(1, 8)
    def _(n):
        band = pl.ds(pl.multiple_of((n - 1) * WINDOW, WINDOW), 2 * WINDOW)
        attend(n, k_v[:, band], v_v[:, band], near)

    for copy in halo_copies:
        copy.wait_recv()
    first_key = jnp.where(s == 0, WINDOW, 0)
    attend(
        0,
        jnp.concatenate([halo_k[...], k_v[:, 0:WINDOW]], axis=1),
        jnp.concatenate([halo_v[...], v_v[:, 0:WINDOW]], axis=1),
        near & (key_at >= first_key),
    )

    def att_rows(yy, cc, low=0, count=HEADS):
        row = (yy * 2 + cc) * HEADS + low
        return att_all.at[pl.ds(pl.multiple_of(row, 32), count)]

    def att_copy(index, ref, target):
        return remote(ref, ref, att_send.at[index], att_recv.at[index], target)

    def att_arrived(index, ref):
        att_copy(index, ref, partner).wait_recv()

    for d, by in DIRS:
        start(att_copy(d, att_rows(y, c), y_next[by]))
    start(att_copy(4, att_rows(y, c), partner))
    w_pass_on()
    up_gather.second()

    for i, copy in enumerate(locals_[3:]):
        copy.wait()

    def mix(yy, first):
        rows = pl.ds(pl.multiple_of(yy * 2 * HEADS, 2 * HEADS), 2 * HEADS)

        @pl.loop(0, ROWS // TILE)
        def _(i):
            tokens = pl.ds(pl.multiple_of(i * TILE, TILE), TILE)
            part = dot(att_all[rows, tokens], w_all[rows, :], ((0,), (0,)))
            mixed[tokens, :] = part if first else mixed[tokens, :] + part

    att_arrived(4, att_rows(y, 1 - c))
    w_arrived(0, w_rows(y, 1 - c))
    mix(y, True)
    up_gather.forward(0)
    up_gather.third()
    for d, by in DIRS:
        att_arrived(d, att_rows(ring(y, -by), c))
        start(att_copy(2 + d, att_rows(ring(y, -by), c, d * HALF, HALF), y_next[by]))
        start(att_copy(5 + d, att_rows(ring(y, -by), c), partner))
    for d, by in DIRS:
        att_arrived(5 + d, att_rows(ring(y, -by), 1 - c))
        for cc in (0, 1):
            w_arrived(1 + 2 * d + cc, w_rows(ring(y, -by), cc))
        mix(ring(y, -by), False)
    up_gather.forward(1)
    for d, by in DIRS:
        att_arrived(2 + d, att_rows(ring(y, 2), c, d * HALF, HALF))
    start(att_copy(7, att_rows(ring(y, 2), c), partner))
    att_arrived(7, att_rows(ring(y, 2), 1 - c))
    for d, by in DIRS:
        for cc in (0, 1):
            w_arrived(7 + 2 * d + cc, w_rows(ring(y, 2), cc, d * HALF, HALF))
    mix(ring(y, 2), False)

    lanes_of = lambda cc: pl.ds(pl.multiple_of(cc * FEATURES, 128), FEATURES)

    def x_block(yy, cc, low=0, count=ROWS):
        return x_all.at[pl.ds(pl.multiple_of(yy * ROWS + low, 512), count), lanes_of(cc)]

    gains = gain[...].astype(F32).reshape(1, FEATURES)
    ones = jnp.ones((8, FEATURES), BF16)
    sq_rows = pl.ds(pl.multiple_of(t * 8, 8), 8)

    @pl.loop(0, ROWS // TILE)
    def _(i):
        tokens = pl.ds(pl.multiple_of(i * TILE, TILE), TILE)
        here = (res_v[tokens, :].astype(F32) + mixed[tokens, :]).astype(BF16)
        stream[tokens, :] = here
        wide = here.astype(F32)
        x_all[pl.ds(pl.multiple_of(y * ROWS + i * TILE, TILE), TILE), lanes_of(c)] = (wide * gains).astype(BF16)
        sq = wide * wide
        high = sq.astype(BF16)
        low = (sq - high.astype(F32)).astype(BF16)
        squares[sq_rows, tokens] = dot(ones, high, ((1,), (1,))) + dot(ones, low, ((1,), (1,)))

    def x_copy(index, ref, target):
        return remote(ref, ref, x_send.at[index], x_recv.at[index], target)

    def x_arrived(index, ref):
        x_copy(index, ref, partner).wait_recv()

    for part in (0, 1):
        for d, by in DIRS:
            start(x_copy(2 * part + d, x_block(y, c, part * 512, 512), y_next[by]))
    start(x_copy(6, x_block(y, c), partner))
    sq_copies = []
    for k in range(1, 8):
        ref = squares.at[sq_rows]
        copy = remote(ref, ref, sq_send.at[k - 1], sq_recv.at[k - 1], (s, (t + k) % 8))
        start(copy)
        sq_copies.append(copy)

    up_gather.forward(2)
    up_gather.forward(3)
    down_gather.first()
    x_arrived(0, x_block(ring(y, -1), c, 0, 512))
    start(x_copy(4, x_block(ring(y, -1), c, 0, 512), y_next[1]))
    x_arrived(1, x_block(ring(y, 1), c, 0, 512))
    x_arrived(3, x_block(ring(y, 1), c, 512, 512))
    start(x_copy(5, x_block(ring(y, 1), c, 512, 512), y_next[-1]))
    x_arrived(2, x_block(ring(y, -1), c, 512, 512))
    start(x_copy(7, x_block(ring(y, -1), c), partner))
    start(x_copy(8, x_block(ring(y, 1), c), partner))

    def hide(yy, first, last):
        @pl.loop(0, ROWS // TILE)
        def _(i):
            tokens = pl.ds(pl.multiple_of(i * TILE, TILE), TILE)
            block = x_all[pl.ds(pl.multiple_of(yy * ROWS + i * TILE, TILE), TILE), :]
            for n in range(3):
                cols = pl.ds(n * 512, 512)
                part = dot(block, up_all[pl.ds(pl.multiple_of(yy * 768, 768), 768), cols], ((1,), (0,)))
                if not first:
                    part = part + hidden[tokens, cols]
                if last:
                    units = jnp.square(jnp.maximum(part, 0.0)).astype(BF16)
                    act_t[cols, tokens] = jnp.transpose(units)
                else:
                    hidden[tokens, cols] = part

    for j in range(4):
        up_gather.last(j)
    x_arrived(6, x_block(y, 1 - c))
    hide(y, True, False)
    for d, by in DIRS:
        x_arrived(7 + d, x_block(ring(y, -by), 1 - c))
        hide(ring(y, -by), False, False)
        if d == 0:
            down_gather.second()
    x_arrived(4, x_block(ring(y, 2), c, 0, 512))
    x_arrived(5, x_block(ring(y, 2), c, 512, 512))
    start(x_copy(9, x_block(ring(y, 2), c), partner))
    x_arrived(9, x_block(ring(y, 2), 1 - c))
    hide(ring(y, 2), False, True)

    GROUPS = (
        [(0, 0, j) for j in range(4)],
        [(1, 0, j) for j in range(4)],
        [(0, i, j) for j in (0, 1) for i in (1, 2)],
        [(1, i, j) for j in (0, 1) for i in (1, 2)],
        [(0, i, j) for j in (2, 3) for i in (1, 2)],
        [(1, i, j) for j in (2, 3) for i in (1, 2)],
        [(half, 3, j) for half in (0, 1) for j in (0, 1)],
        [(half, 3, j) for half in (0, 1) for j in (2, 3)],
    )

    class Piece:
        def __init__(self, half, i, j):
            sec, prim = down_gather.at(half)
            sec, prim = ring(sec, STEPS[i]), ring(prim, STEPS[j])
            zz, xx = (sec, prim) if half == 0 else (prim, sec)
            self.row = (zz * 4 + xx) * SHARD + half * HALF
            self.part = (xx % 2) * 2 + half
            self.mine = xx // 2 == c
            self.away = (y - zz + 4) % 4
            self.pair = zz * 4 + self.part

        def rows(self, low=0, count=HALF):
            return pl.ds(pl.multiple_of(self.row + low, 16), count)

        def paired_rows(self, low=0, count=HALF):
            return pl.ds(pl.multiple_of(self.pair * HALF + low, 16), count)

        def to_pair(self):
            return remote(
                partials.at[self.rows()], paired.at[self.paired_rows()],
                pair_send.at[self.pair], pair_recv.at[self.pair], partner,
            )

        def hop(self, step, k, by):
            index = step * 8 + k * 4 + self.part
            if step < 2:
                dst = chained.at[pl.ds(pl.multiple_of(index * QUARTER, 16), QUARTER)]
            else:
                dst = final.at[pl.ds(pl.multiple_of(self.part * HALF + k * QUARTER, 16), QUARTER)]
            return remote(
                partials.at[self.rows(k * QUARTER, QUARTER)], dst,
                chain_send.at[index], chain_recv.at[index], y_next[by],
            )

        def add_pair(self, k):
            rows = self.rows(k * QUARTER, QUARTER)
            total = partials[rows, :].astype(F32) + paired[self.paired_rows(k * QUARTER, QUARTER), :].astype(F32)
            partials[rows, :] = total.astype(BF16)

        def add_hop(self, step, k):
            rows = self.rows(k * QUARTER, QUARTER)
            there = pl.ds(pl.multiple_of((step * 8 + k * 4 + self.part) * QUARTER, 16), QUARTER)
            total = partials[rows, :].astype(F32) + chained[there, :].astype(F32)
            partials[rows, :] = total.astype(BF16)

    groups = [[Piece(*facts) for facts in group] for group in GROUPS]

    def compute(group):
        @pl.loop(0, ROWS // TILE)
        def _(i):
            tokens = pl.ds(pl.multiple_of(i * TILE, TILE), TILE)
            weight = jnp.concatenate([down_all[p.rows(), :] for p in group], axis=0)
            part = dot(weight, act_t[:, tokens], ((1,), (0,))).astype(BF16)
            for k, p in enumerate(group):
                partials[p.rows(), tokens] = part[k * HALF : (k + 1) * HALF]

        for p in group:
            @pl.when(jnp.logical_not(p.mine))
            def _():
                p.to_pair().start()

    def combine(group):
        for p in group:
            @pl.when(p.mine & (p.away != 0))
            def _():
                p.to_pair().wait_recv()
                for k in (0, 1):
                    p.add_pair(k)
                for k, by in DIRS:
                    @pl.when(p.away == (1 if k == 0 else 3))
                    def _():
                        p.hop(0, k, by).start()

    def relay(group):
        for p in group:
            @pl.when(p.mine & (p.away == 2))
            def _():
                for k, by in DIRS:
                    p.hop(0, k, by).wait_recv()
                    p.add_hop(0, k)
                    p.hop(1, k, by).start()

    def deliver(group):
        for p in group:
            for k, by in DIRS:
                @pl.when(p.mine & (p.away == (3 if k == 0 else 1)))
                def _():
                    p.hop(1, k, by).wait_recv()
                    p.add_hop(1, k)
                    p.hop(2, k, by).start()

    down_gather.forward(0)
    down_gather.third()
    compute(groups[0])
    compute(groups[1])
    combine(groups[0])
    combine(groups[1])
    down_gather.forward(1)
    compute(groups[2])
    relay(groups[0])
    compute(groups[3])
    relay(groups[1])
    combine(groups[2])
    combine(groups[3])
    deliver(groups[0])
    deliver(groups[1])
    down_gather.forward(2)
    relay(groups[2])
    relay(groups[3])
    down_gather.forward(3)
    compute(groups[4])
    deliver(groups[2])
    compute(groups[5])
    combine(groups[4])
    combine(groups[5])
    deliver(groups[3])
    down_gather.last(0)
    down_gather.last(1)
    compute(groups[6])
    relay(groups[4])
    relay(groups[5])
    combine(groups[6])
    deliver(groups[4])
    deliver(groups[5])
    down_gather.last(2)
    down_gather.last(3)
    compute(groups[7])
    relay(groups[6])
    combine(groups[7])
    deliver(groups[6])
    relay(groups[7])
    deliver(groups[7])

    for copy in sq_copies:
        copy.wait_recv()
    own = [Piece(half, 0, 0) for half in (0, 1, 0, 1)]
    for part, p in enumerate(own):
        p.part = part
        p.row = (y * 4 + c * 2) * SHARD + part * HALF
        p.pair = y * 4 + part
    for p in own:
        p.to_pair().wait_recv()
        for k, by in DIRS:
            p.hop(2, k, by).wait_recv()
    mine = pl.ds(pl.multiple_of((y * 4 + c * 2) * SHARD, FEATURES), FEATURES)
    beside = pl.ds(pl.multiple_of(y * FEATURES, FEATURES), FEATURES)

    @pl.loop(0, ROWS // 128)
    def _(i):
        tokens = pl.ds(pl.multiple_of(i * 128, 128), 128)
        total = partials[mine, tokens].astype(F32) + paired[beside, tokens].astype(F32)
        total = total + final[:, tokens].astype(F32)
        norm = squares[0:1, tokens]
        for k in range(1, 8):
            norm = norm + squares[8 * k : 8 * k + 1, tokens]
        total = total * (1.0 / (norm * (1.0 / D) + EPSILON))
        out_v[tokens, :] = (stream[tokens, :].astype(F32) + jnp.transpose(total)).astype(BF16)

    store = pltpu.make_async_copy(out_v, result, local_sem.at[7])
    store.start()
    for copy in pending:
        copy.wait_send()
    for k in range(16):
        p = own[0]
        p.pair = k
        p.to_pair().wait_send()
    for p in own:
        for k, by in DIRS:
            for step in range(3):
                p.hop(step, k, by).wait_send()
    store.wait()


def body(
    queries, key_heads, projected_value_heads, sink_logit_table, out_weight,
    residual, norm_gain, up_weight, down_weight,
):
    hbm = pl.BlockSpec(memory_space=pl.ANY)
    dma = pltpu.SemaphoreType.DMA
    return pl.pallas_call(
        kernel,
        out_shape=jax.ShapeDtypeStruct((ROWS, FEATURES), BF16),
        in_specs=[hbm, hbm, hbm, pl.BlockSpec(memory_space=pltpu.SMEM), hbm, hbm,
                  pl.BlockSpec(memory_space=pltpu.VMEM), hbm, hbm],
        out_specs=hbm,
        scratch_shapes=[
            pltpu.VMEM((D, HIDDEN), BF16),
            pltpu.VMEM((D, HIDDEN), BF16),
            pltpu.VMEM((4 * ROWS, 2 * FEATURES), BF16),
            pltpu.VMEM((8 * HEADS, ROWS), BF16),
            pltpu.VMEM((8 * HEADS, FEATURES), BF16),
            pltpu.VMEM((2, HALF, 2 * FEATURES), BF16),
            pltpu.VMEM((ROWS, HIDDEN), F32),
            pltpu.VMEM((HIDDEN, ROWS), BF16),
            pltpu.VMEM((ROWS, FEATURES), F32),
            pltpu.VMEM((ROWS, FEATURES), BF16),
            pltpu.VMEM((ROWS, FEATURES), BF16),
            pltpu.VMEM((HEADS, ROWS), BF16),
            pltpu.VMEM((HEAD_SIZE, ROWS), BF16),
            pltpu.VMEM((HEAD_SIZE, ROWS), BF16),
            pltpu.VMEM((HEAD_SIZE, WINDOW), BF16),
            pltpu.VMEM((HEAD_SIZE, WINDOW), BF16),
            pltpu.VMEM((D, ROWS), BF16),
            pltpu.VMEM((D // 2, ROWS), BF16),
            pltpu.VMEM((16 * QUARTER, ROWS), BF16),
            pltpu.VMEM((FEATURES, ROWS), BF16),
            pltpu.VMEM((64, ROWS), F32),
            pltpu.VMEM((ROWS, FEATURES), BF16),
            dma((8,)), dma((11,)), dma((11,)), dma((2,)), dma((2,)), dma((80,)), dma((80,)),
            dma((8,)), dma((8,)), dma((10,)), dma((10,)), dma((7,)), dma((7,)),
            dma((16,)), dma((16,)), dma((24,)), dma((24,)),
        ],
        compiler_params=pltpu.CompilerParams(
            collective_id=0, has_side_effects=True, vmem_limit_bytes=67043328
        ),
    )(
        queries.T, key_heads.T, projected_value_heads.T, sink_logit_table, out_weight,
        residual, norm_gain, up_weight, down_weight.T,
    )


def solution(mesh):
    return jax.shard_map(
        body,
        mesh=mesh,
        in_specs=(
            P("sp", "tp"), P("sp", "tp"), P("sp", "tp"), P("tp"), P("tp", None),
            P("sp", "tp"), P("tp"), P("sp", "tp"), P("tp", "sp"),
        ),
        out_specs=P("sp", "tp"),
        check_vma=False,
    )
```

```python
import functools

import jax
import jax.numpy as jnp
from jax import lax
from jax.experimental import pallas as pl
from jax.experimental.pallas import tpu as pltpu
from jax.sharding import PartitionSpec as P

D = 3072
HEAD_SIZE = 64
WINDOW = 128
EPSILON = 1e-06

ROWS = 1024
FEATURES = 384
HEADS = 192
SHARD = 192
HALF = 96
QUARTER = 48
HIDDEN = 1536
TILE = 256

MESH = pl.DeviceIdType.MESH
BF16 = jnp.bfloat16
F32 = jnp.float32


def dot(a, b, dims):
    return lax.dot_general(a, b, (dims, ((), ())), preferred_element_type=F32)


def kernel(
    queries, keys, values, sinks_in, out_weight, residual, gains_in, up, down,
    result,
    up_all, down_all, x_all, att_all, w_all, w_pass, hidden, act_t, mixed, stream, res_v,
    q_v, k_v, v_v, halo_k, halo_v, partials, paired, final, squares, sink, gain,
    local_sem, w_send, w_recv, halo_send, halo_recv, g_send, g_recv,
    att_send, att_recv, x_send, x_recv, sq_send, sq_recv,
    pair_send, pair_recv, owner_send, owner_recv,
):
    s, t = lax.axis_index("sp"), lax.axis_index("tp")
    z, x = s // 4, s % 4
    y, c = t // 2, t % 2

    def ring(position, by):
        return (position + by + 4) % 4

    def device(zz, xx, yy, cc):
        return (zz * 4 + xx, yy * 2 + cc)

    partner = (s, y * 2 + (1 - c))
    y_next = {1: (s, ring(y, 1) * 2 + c), -1: (s, ring(y, -1) * 2 + c)}
    DIRS = ((0, 1), (1, -1))

    def remote(src, dst, send, recv, target):
        return pltpu.make_async_remote_copy(
            src_ref=src, dst_ref=dst, send_sem=send, recv_sem=recv,
            device_id=target, device_id_type=MESH,
        )

    pending = []

    def start(copy):
        copy.start()
        pending.append(copy)

    barrier = pltpu.get_barrier_semaphore()
    greeted = [
        device(z, ring(x, 1), y, c), device(z, ring(x, -1), y, c),
        device(ring(z, 1), x, y, c), device(ring(z, -1), x, y, c),
        ((s + 1) % 16, t), ((s + 15) % 16, t),
    ] + [(s, (t + k) % 8) for k in range(1, 8)]
    for other in greeted:
        pl.semaphore_signal(barrier, inc=1, device_id=other, device_id_type=MESH)
    locals_ = [
        pltpu.make_async_copy(src, dst, local_sem.at[i])
        for i, (src, dst) in enumerate([
            (queries, q_v), (keys, k_v), (values, v_v), (sinks_in, sink), (gains_in, gain), (residual, res_v),
            (up, up_all.at[pl.ds(pl.multiple_of(s * SHARD, SHARD), SHARD)]),
            (down, down_all.at[pl.ds(pl.multiple_of(s * SHARD, SHARD), SHARD)]),
            (out_weight.at[:, pl.ds(pl.multiple_of(t * FEATURES, 128), FEATURES)],
             w_all.at[pl.ds(pl.multiple_of(t * HEADS, HEADS), HEADS)]),
        ])
    ]
    for copy in locals_:
        copy.start()
    pl.semaphore_wait(barrier, len(greeted))

    STEPS = (0, -1, 1, 2)
    ORDER = ((0, 1, 2, 3), (0, 1, 3, 2))

    class Gather:
        def __init__(self, own, buf, base):
            self.own, self.buf, self.base = own, buf, base

        def spot(self, half, sec, prim, low, count):
            zz, xx = (sec, prim) if half == 0 else (prim, sec)
            row = (zz * 4 + xx) * SHARD + half * HALF + low
            return self.buf.at[pl.ds(pl.multiple_of(row, 16), count)]

        def copy(self, half, index, src, dst, target):
            k = self.base + half * 20 + index
            return remote(src, dst, g_send.at[k], g_recv.at[k], target)

        def at(self, half):
            return (z, x) if half == 0 else (x, z)

        def towards(self, half, primary, by):
            if primary == (half == 0):
                return device(z, ring(x, by), y, c)
            return device(ring(z, by), x, y, c)

        def first(self):
            for half in (0, 1):
                sec, prim = self.at(half)
                src = self.own.at[pl.ds(half * HALF, HALF)]
                dst = self.spot(half, sec, prim, 0, HALF)
                for d, by in DIRS:
                    start(self.copy(half, d, src, dst, self.towards(half, True, by)))
            for half in (0, 1):
                sec, prim = self.at(half)
                src = self.own.at[pl.ds(half * HALF, HALF)]
                dst = self.spot(half, sec, prim, 0, HALF)
                for d, by in DIRS:
                    start(self.copy(half, 4 + d, src, dst, self.towards(half, False, by)))

        def wait(self, half, index, sec, prim, low, count):
            ref = self.spot(half, sec, prim, low, count)
            self.copy(half, index, ref, ref, partner).wait_recv()

        def second(self):
            for half in (0, 1):
                sec, prim = self.at(half)
                for d, by in DIRS:
                    origin = ring(prim, -by)
                    self.wait(half, d, sec, origin, 0, HALF)
                    piece = self.spot(half, sec, origin, d * QUARTER, QUARTER)
                    start(self.copy(half, 2 + d, piece, piece, self.towards(half, True, by)))
            for half in (0, 1):
                self.spread(half, 1)

        def spread(self, half, j):
            sec, prim = self.at(half)
            piece = self.spot(half, sec, ring(prim, STEPS[j]), 0, HALF)
            for d, by in DIRS:
                start(self.copy(half, 4 + 2 * j + d, piece, piece, self.towards(half, False, by)))

        def opposite(self, half):
            sec, prim = self.at(half)
            for d, by in DIRS:
                self.wait(half, 2 + d, sec, ring(prim, 2), d * QUARTER, QUARTER)
            self.spread(half, 3)

        def third(self):
            self.spread(0, 2)
            self.opposite(1)

        def fourth(self):
            self.spread(1, 2)
            self.opposite(0)

        def forward(self, k):
            for half in (0, 1):
                j = ORDER[half][k]
                sec, prim = self.at(half)
                origin = ring(prim, STEPS[j])
                for d, by in DIRS:
                    self.wait(half, 4 + 2 * j + d, ring(sec, -by), origin, 0, HALF)
                    piece = self.spot(half, ring(sec, -by), origin, d * QUARTER, QUARTER)
                    start(self.copy(half, 12 + 2 * j + d, piece, piece, self.towards(half, False, by)))

        def last(self, k):
            for half in (0, 1):
                j = ORDER[half][k]
                sec, prim = self.at(half)
                origin = ring(prim, STEPS[j])
                for d, by in DIRS:
                    self.wait(half, 12 + 2 * j + d, ring(sec, 2), origin, d * QUARTER, QUARTER)

    up_gather = Gather(up, up_all, 0)
    down_gather = Gather(down, down_all, 40)
    after = ((s + 1) % 16, t)
    tail = pl.ds(ROWS - WINDOW, WINDOW)
    halo_copies = [
        remote(keys.at[:, tail], halo_k, halo_send.at[0], halo_recv.at[0], after),
        remote(values.at[:, tail], halo_v, halo_send.at[1], halo_recv.at[1], after),
    ]
    for copy in halo_copies:
        start(copy)
    up_gather.first()

    def w_cols(yy, cc=0, count=FEATURES):
        return pl.ds(pl.multiple_of((yy * 2 + cc) * FEATURES, 128), count)

    def w_rows(yy, cc, low=0, count=HEADS):
        return w_all.at[pl.ds(pl.multiple_of((yy * 2 + cc) * HEADS + low, 32), count)]

    def w_relay(k, by):
        src = out_weight.at[pl.ds(k * HALF, HALF), w_cols(ring(y, 2), 0, 2 * FEATURES)]
        return remote(src, w_pass.at[k], w_send.at[5 + k], w_recv.at[5 + k], y_next[by])

    for k, by in DIRS:
        start(w_relay(k, by))
    start(remote(out_weight.at[:, w_cols(y, 1 - c)], w_rows(y, c), w_send.at[0], w_recv.at[0], partner))
    for k, by in DIRS:
        for cc in (0, 1):
            start(remote(
                out_weight.at[:, w_cols(ring(y, by), cc)], w_rows(y, c),
                w_send.at[1 + 2 * k + cc], w_recv.at[1 + 2 * k + c], (s, ring(y, by) * 2 + cc),
            ))

    def w_arrived(index, ref):
        remote(ref, ref, w_send.at[index], w_recv.at[index], partner).wait_recv()

    def w_pass_on():
        for k, by in DIRS:
            w_relay(k, by).wait_recv()
            for cc in (0, 1):
                start(remote(
                    w_pass.at[k, :, pl.ds(cc * FEATURES, FEATURES)], w_rows(ring(y, -by), c, k * HALF, HALF),
                    w_send.at[7 + 2 * k + cc], w_recv.at[7 + 2 * k + c], (s, ring(y, by) * 2 + cc),
                ))

    key_at = lax.broadcasted_iota(jnp.int32, (2 * WINDOW, 3 * WINDOW), 0)
    query_at = lax.broadcasted_iota(jnp.int32, (2 * WINDOW, 3 * WINDOW), 1) % WINDOW
    mine_row = t * HEADS

    def attend(n, key_band, value_band, allowed):
        lanes = pl.ds(pl.multiple_of(n * WINDOW, WINDOW), WINDOW)
        q = jnp.concatenate([q_v[pl.ds(g * HEAD_SIZE, HEAD_SIZE), lanes] for g in range(3)], axis=1)
        scores = dot(key_band, q, ((0,), (0,))) * HEAD_SIZE**-0.5
        masked = jnp.where(allowed, scores, -1e30)
        top = jnp.maximum(jnp.max(masked, axis=0, keepdims=True), sinks)
        powers = jnp.where(allowed, jnp.exp(masked - top), 0.0)
        denom = jnp.sum(powers, axis=0, keepdims=True) + jnp.exp(sinks - top)
        probs = (powers * (1.0 / denom)).astype(BF16)
        output = dot(value_band, probs, ((1,), (0,))).astype(BF16)
        for g in range(3):
            rows = pl.ds(pl.multiple_of(mine_row + g * HEAD_SIZE, HEAD_SIZE), HEAD_SIZE)
            att_all[rows, lanes] = output[:, g * WINDOW : (g + 1) * WINDOW]

    near = (key_at > query_at) & (key_at <= query_at + WINDOW)
    for copy in locals_[:4]:
        copy.wait()
    sinks = jnp.concatenate([jnp.full((1, WINDOW), sink[g], F32) for g in range(3)], axis=1)

    @pl.loop(1, 8)
    def _(n):
        band = pl.ds(pl.multiple_of((n - 1) * WINDOW, WINDOW), 2 * WINDOW)
        attend(n, k_v[:, band], v_v[:, band], near)

    for copy in halo_copies:
        copy.wait_recv()
    first_key = jnp.where(s == 0, WINDOW, 0)
    attend(
        0,
        jnp.concatenate([halo_k[...], k_v[:, 0:WINDOW]], axis=1),
        jnp.concatenate([halo_v[...], v_v[:, 0:WINDOW]], axis=1),
        near & (key_at >= first_key),
    )

    def att_rows(yy, cc, low=0, count=HEADS):
        row = (yy * 2 + cc) * HEADS + low
        return att_all.at[pl.ds(pl.multiple_of(row, 32), count)]

    def att_copy(index, ref, target):
        return remote(ref, ref, att_send.at[index], att_recv.at[index], target)

    def att_arrived(index, ref):
        att_copy(index, ref, partner).wait_recv()

    for d, by in DIRS:
        start(att_copy(d, att_rows(y, c), y_next[by]))
    start(att_copy(4, att_rows(y, c), partner))
    w_pass_on()
    up_gather.second()

    for copy in locals_[4:]:
        copy.wait()

    def mix(yy, first):
        rows = pl.ds(pl.multiple_of(yy * 2 * HEADS, 2 * HEADS), 2 * HEADS)

        @pl.loop(0, ROWS // TILE)
        def _(i):
            tokens = pl.ds(pl.multiple_of(i * TILE, TILE), TILE)
            part = dot(att_all[rows, tokens], w_all[rows, :], ((0,), (0,)))
            mixed[tokens, :] = part if first else mixed[tokens, :] + part

    att_arrived(4, att_rows(y, 1 - c))
    w_arrived(0, w_rows(y, 1 - c))
    mix(y, True)
    up_gather.forward(0)
    up_gather.third()
    for d, by in DIRS:
        att_arrived(d, att_rows(ring(y, -by), c))
        start(att_copy(2 + d, att_rows(ring(y, -by), c, d * HALF, HALF), y_next[by]))
        start(att_copy(5 + d, att_rows(ring(y, -by), c), partner))
    for d, by in DIRS:
        att_arrived(5 + d, att_rows(ring(y, -by), 1 - c))
        for cc in (0, 1):
            w_arrived(1 + 2 * d + cc, w_rows(ring(y, -by), cc))
        mix(ring(y, -by), False)
    up_gather.forward(1)
    up_gather.fourth()
    for d, by in DIRS:
        att_arrived(2 + d, att_rows(ring(y, 2), c, d * HALF, HALF))
    start(att_copy(7, att_rows(ring(y, 2), c), partner))
    att_arrived(7, att_rows(ring(y, 2), 1 - c))
    for d, by in DIRS:
        for cc in (0, 1):
            w_arrived(7 + 2 * d + cc, w_rows(ring(y, 2), cc, d * HALF, HALF))
    mix(ring(y, 2), False)

    lanes_of = lambda cc: pl.ds(pl.multiple_of(cc * FEATURES, 128), FEATURES)

    def x_block(yy, cc, low=0, count=ROWS):
        return x_all.at[pl.ds(pl.multiple_of(yy * ROWS + low, 512), count), lanes_of(cc)]

    gains = gain[...].astype(F32).reshape(1, FEATURES)
    ones = jnp.ones((8, FEATURES), BF16)
    sq_rows = pl.ds(pl.multiple_of(t * 8, 8), 8)

    @pl.loop(0, ROWS // TILE)
    def _(i):
        tokens = pl.ds(pl.multiple_of(i * TILE, TILE), TILE)
        here = (res_v[tokens, :].astype(F32) + mixed[tokens, :]).astype(BF16)
        stream[tokens, :] = here
        wide = here.astype(F32)
        x_all[pl.ds(pl.multiple_of(y * ROWS + i * TILE, TILE), TILE), lanes_of(c)] = (wide * gains).astype(BF16)
        sq = wide * wide
        high = sq.astype(BF16)
        low = (sq - high.astype(F32)).astype(BF16)
        squares[sq_rows, tokens] = dot(ones, high, ((1,), (1,))) + dot(ones, low, ((1,), (1,)))

    def x_copy(index, ref, target):
        return remote(ref, ref, x_send.at[index], x_recv.at[index], target)

    def x_arrived(index, ref):
        x_copy(index, ref, partner).wait_recv()

    for part in (0, 1):
        for d, by in DIRS:
            start(x_copy(2 * part + d, x_block(y, c, part * 512, 512), y_next[by]))
    start(x_copy(6, x_block(y, c), partner))
    sq_copies = []
    for k in range(1, 8):
        ref = squares.at[sq_rows]
        copy = remote(ref, ref, sq_send.at[k - 1], sq_recv.at[k - 1], (s, (t + k) % 8))
        start(copy)
        sq_copies.append(copy)

    up_gather.forward(2)
    x_arrived(0, x_block(ring(y, -1), c, 0, 512))
    start(x_copy(4, x_block(ring(y, -1), c, 0, 512), y_next[1]))
    x_arrived(1, x_block(ring(y, 1), c, 0, 512))
    up_gather.forward(3)
    down_gather.first()
    x_arrived(3, x_block(ring(y, 1), c, 512, 512))
    start(x_copy(5, x_block(ring(y, 1), c, 512, 512), y_next[-1]))
    x_arrived(2, x_block(ring(y, -1), c, 512, 512))
    start(x_copy(7, x_block(ring(y, -1), c), partner))
    start(x_copy(8, x_block(ring(y, 1), c), partner))

    def hide(yy, first, last):
        @pl.loop(0, ROWS // TILE)
        def _(i):
            tokens = pl.ds(pl.multiple_of(i * TILE, TILE), TILE)
            block = x_all[pl.ds(pl.multiple_of(yy * ROWS + i * TILE, TILE), TILE), :]
            for n in range(3):
                cols = pl.ds(n * 512, 512)
                part = dot(block, up_all[pl.ds(pl.multiple_of(yy * 768, 768), 768), cols], ((1,), (0,)))
                if not first:
                    part = part + hidden[tokens, cols]
                if last:
                    units = jnp.square(jnp.maximum(part, 0.0)).astype(BF16)
                    act_t[cols, tokens] = jnp.transpose(units)
                else:
                    hidden[tokens, cols] = part

    for j in range(4):
        up_gather.last(j)
    x_arrived(6, x_block(y, 1 - c))
    hide(y, True, False)
    for d, by in DIRS:
        x_arrived(7 + d, x_block(ring(y, -by), 1 - c))
        hide(ring(y, -by), False, False)
        if d == 0:
            down_gather.second()
    x_arrived(4, x_block(ring(y, 2), c, 0, 512))
    x_arrived(5, x_block(ring(y, 2), c, 512, 512))
    start(x_copy(9, x_block(ring(y, 2), c), partner))
    x_arrived(9, x_block(ring(y, 2), 1 - c))
    hide(ring(y, 2), False, True)

    GROUPS = [[(half, 0, j) for j in range(4)] for half in (0, 1)]
    for k in range(4):
        GROUPS.append([(half, i, ORDER[half][k]) for half in (0, 1) for i in (1, 2)])
        GROUPS.append([(half, 3, ORDER[half][k]) for half in (0, 1)])

    class Piece:
        def __init__(self, half, i, j):
            sec, prim = down_gather.at(half)
            sec, prim = ring(sec, STEPS[i]), ring(prim, STEPS[j])
            zz, xx = (sec, prim) if half == 0 else (prim, sec)
            self.row = (zz * 4 + xx) * SHARD + half * HALF
            self.part = (xx % 2) * 2 + half
            self.mine = xx // 2 == c
            self.away = (y - zz + 4) % 4
            self.pair = zz * 4 + self.part

        def rows(self, low=0, count=HALF):
            return pl.ds(pl.multiple_of(self.row + low, 16), count)

        def paired_rows(self, low=0, count=HALF):
            return pl.ds(pl.multiple_of(self.pair * HALF + low, 16), count)

        def to_pair(self):
            return remote(
                partials.at[self.rows()], paired.at[self.paired_rows()],
                pair_send.at[self.pair], pair_recv.at[self.pair], partner,
            )

        def to_owner(self):
            index = (self.away - 1) * 4 + self.part
            return remote(
                partials.at[self.rows()], final.at[pl.ds(pl.multiple_of(index * HALF, 32), HALF)],
                owner_send.at[index], owner_recv.at[index], (s, ring(y, -self.away) * 2 + c),
            )

        def add_pair(self, k):
            rows = self.rows(k * QUARTER, QUARTER)
            total = partials[rows, :].astype(F32) + paired[self.paired_rows(k * QUARTER, QUARTER), :].astype(F32)
            partials[rows, :] = total.astype(BF16)

    groups = [[Piece(*facts) for facts in group] for group in GROUPS]

    def compute(group):
        @pl.loop(0, ROWS // TILE)
        def _(i):
            tokens = pl.ds(pl.multiple_of(i * TILE, TILE), TILE)
            weight = jnp.concatenate([down_all[p.rows(), :] for p in group], axis=0)
            part = dot(weight, act_t[:, tokens], ((1,), (0,))).astype(BF16)
            for k, p in enumerate(group):
                partials[p.rows(), tokens] = part[k * HALF : (k + 1) * HALF]

        for p in group:
            @pl.when(jnp.logical_not(p.mine))
            def _():
                p.to_pair().start()

    def combine(group):
        for p in group:
            @pl.when(p.mine & (p.away != 0))
            def _():
                p.to_pair().wait_recv()
                for k in (0, 1):
                    p.add_pair(k)
                p.to_owner().start()

    down_gather.forward(0)
    down_gather.third()
    compute(groups[2])
    compute(groups[1])
    combine(groups[2])
    down_gather.forward(1)
    down_gather.fourth()
    compute(groups[0])
    combine(groups[1])
    compute(groups[4])
    combine(groups[0])
    down_gather.last(0)
    compute(groups[3])
    combine(groups[4])
    combine(groups[3])
    down_gather.forward(2)
    compute(groups[6])
    combine(groups[6])
    down_gather.last(1)
    compute(groups[5])
    combine(groups[5])
    down_gather.forward(3)
    compute(groups[8])
    combine(groups[8])
    down_gather.last(2)
    compute(groups[7])
    combine(groups[7])
    down_gather.last(3)
    compute(groups[9])
    combine(groups[9])

    for copy in sq_copies:
        copy.wait_recv()
    own = [Piece(half, 0, 0) for half in (0, 1, 0, 1)]
    for part, p in enumerate(own):
        p.part = part
        p.row = (y * 4 + c * 2) * SHARD + part * HALF
        p.pair = y * 4 + part
    for p in own:
        p.to_pair().wait_recv()
        for away in (1, 2, 3):
            p.away = away
            p.to_owner().wait_recv()
    mine = pl.ds(pl.multiple_of((y * 4 + c * 2) * SHARD, FEATURES), FEATURES)
    beside = pl.ds(pl.multiple_of(y * FEATURES, FEATURES), FEATURES)

    @pl.loop(0, ROWS // 128)
    def _(i):
        tokens = pl.ds(pl.multiple_of(i * 128, 128), 128)
        total = partials[mine, tokens].astype(F32) + paired[beside, tokens].astype(F32)
        for k in range(3):
            total = total + final[k * FEATURES : (k + 1) * FEATURES, tokens].astype(F32)
        norm = squares[0:1, tokens]
        for k in range(1, 8):
            norm = norm + squares[8 * k : 8 * k + 1, tokens]
        total = total * (1.0 / (norm * (1.0 / D) + EPSILON))
        result[tokens, :] = (stream[tokens, :].astype(F32) + jnp.transpose(total)).astype(BF16)

    for copy in pending:
        copy.wait_send()
    for k in range(16):
        p = own[0]
        p.pair = k
        p.to_pair().wait_send()
    for p in own:
        for away in (1, 2, 3):
            p.away = away
            p.to_owner().wait_send()


def body(
    queries, key_heads, projected_value_heads, sink_logit_table, out_weight,
    residual, norm_gain, up_weight, down_weight,
):
    hbm = pl.BlockSpec(memory_space=pl.ANY)
    dma = pltpu.SemaphoreType.DMA
    return pl.pallas_call(
        kernel,
        out_shape=pltpu.VMEM((ROWS, FEATURES), BF16),
        in_specs=[hbm] * 9,
        out_specs=pl.BlockSpec(memory_space=pltpu.VMEM),
        scratch_shapes=[
            pltpu.VMEM((D, HIDDEN), BF16),
            pltpu.VMEM((D, HIDDEN), BF16),
            pltpu.VMEM((4 * ROWS, 2 * FEATURES), BF16),
            pltpu.VMEM((8 * HEADS, ROWS), BF16),
            pltpu.VMEM((8 * HEADS, FEATURES), BF16),
            pltpu.VMEM((2, HALF, 2 * FEATURES), BF16),
            pltpu.VMEM((ROWS, HIDDEN), F32),
            pltpu.VMEM((HIDDEN, ROWS), BF16),
            pltpu.VMEM((ROWS, FEATURES), F32),
            pltpu.VMEM((ROWS, FEATURES), BF16),
            pltpu.VMEM((ROWS, FEATURES), BF16),
            pltpu.VMEM((HEADS, ROWS), BF16),
            pltpu.VMEM((HEAD_SIZE, ROWS), BF16),
            pltpu.VMEM((HEAD_SIZE, ROWS), BF16),
            pltpu.VMEM((HEAD_SIZE, WINDOW), BF16),
            pltpu.VMEM((HEAD_SIZE, WINDOW), BF16),
            pltpu.VMEM((D, ROWS), BF16),
            pltpu.VMEM((D // 2, ROWS), BF16),
            pltpu.VMEM((3 * FEATURES, ROWS), BF16),
            pltpu.VMEM((64, ROWS), F32),
            pltpu.SMEM((3,), F32),
            pltpu.VMEM((FEATURES,), BF16),
            dma((9,)), dma((11,)), dma((11,)), dma((2,)), dma((2,)), dma((80,)), dma((80,)),
            dma((8,)), dma((8,)), dma((10,)), dma((10,)), dma((7,)), dma((7,)),
            dma((16,)), dma((16,)), dma((12,)), dma((12,)),
        ],
        compiler_params=pltpu.CompilerParams(
            collective_id=0, has_side_effects=True, vmem_limit_bytes=60 * 2**20
        ),
    )(
        queries.T, key_heads.T, projected_value_heads.T, sink_logit_table, out_weight,
        residual, norm_gain, up_weight, down_weight.T,
    )


def solution(mesh):
    return jax.shard_map(
        body,
        mesh=mesh,
        in_specs=(
            P("sp", "tp"), P("sp", "tp"), P("sp", "tp"), P("tp"), P("tp", None),
            P("sp", "tp"), P("tp"), P("sp", "tp"), P("tp", "sp"),
        ),
        out_specs=P("sp", "tp"),
        check_vma=False,
    )
```

```python
import functools

import jax
import jax.numpy as jnp
from jax import lax
from jax.experimental import pallas as pl
from jax.experimental.pallas import tpu as pltpu
from jax.sharding import PartitionSpec as P

D = 3072
HEAD_SIZE = 64
WINDOW = 128
EPSILON = 1e-06

ROWS = 1024
FEATURES = 384
HEADS = 192
SHARD = 192
HALF = 96
QUARTER = 48
HIDDEN = 1536
TILE = 256

MESH = pl.DeviceIdType.MESH
BF16 = jnp.bfloat16
F32 = jnp.float32


def dot(a, b, dims):
    return lax.dot_general(a, b, (dims, ((), ())), preferred_element_type=F32)


def kernel(
    queries, keys, values, sinks_in, out_weight, residual, gains_in, up, down,
    result,
    up_all, down_all, x_all, att_all, w_all, w_pass, hidden, act_t, mixed, stream, res_v,
    q_v, k_v, v_v, halo_k, halo_v, partials, paired, chained, final, squares, sink, gain,
    local_sem, w_send, w_recv, halo_send, halo_recv, g_send, g_recv,
    att_send, att_recv, x_send, x_recv, sq_send, sq_recv,
    pair_send, pair_recv, side_send, side_recv, owner_send, owner_recv,
):
    s, t = lax.axis_index("sp"), lax.axis_index("tp")
    z, x = s // 4, s % 4
    y, c = t // 2, t % 2

    def ring(position, by):
        return (position + by + 4) % 4

    def device(zz, xx, yy, cc):
        return (zz * 4 + xx, yy * 2 + cc)

    partner = (s, y * 2 + (1 - c))
    y_next = {1: (s, ring(y, 1) * 2 + c), -1: (s, ring(y, -1) * 2 + c)}
    DIRS = ((0, 1), (1, -1))

    def remote(src, dst, send, recv, target):
        return pltpu.make_async_remote_copy(
            src_ref=src, dst_ref=dst, send_sem=send, recv_sem=recv,
            device_id=target, device_id_type=MESH,
        )

    pending = []

    def start(copy):
        copy.start()
        pending.append(copy)

    barrier = pltpu.get_barrier_semaphore()
    greeted = [
        device(z, ring(x, 1), y, c), device(z, ring(x, -1), y, c),
        device(ring(z, 1), x, y, c), device(ring(z, -1), x, y, c),
        ((s + 1) % 16, t), ((s + 15) % 16, t),
    ] + [(s, (t + k) % 8) for k in range(1, 8)]
    for other in greeted:
        pl.semaphore_signal(barrier, inc=1, device_id=other, device_id_type=MESH)
    locals_ = [
        pltpu.make_async_copy(src, dst, local_sem.at[i])
        for i, (src, dst) in enumerate([
            (queries, q_v), (keys, k_v), (values, v_v), (sinks_in, sink), (gains_in, gain), (residual, res_v),
            (up, up_all.at[pl.ds(pl.multiple_of(s * SHARD, SHARD), SHARD)]),
            (down, down_all.at[pl.ds(pl.multiple_of(s * SHARD, SHARD), SHARD)]),
            (out_weight.at[:, pl.ds(pl.multiple_of(t * FEATURES, 128), FEATURES)],
             w_all.at[pl.ds(pl.multiple_of(t * HEADS, HEADS), HEADS)]),
        ])
    ]
    for copy in locals_:
        copy.start()
    pl.semaphore_wait(barrier, len(greeted))

    STEPS = (0, -1, 1, 2)
    ORDER = ((0, 1, 2, 3), (0, 1, 3, 2))

    class Gather:
        def __init__(self, own, buf, base):
            self.own, self.buf, self.base = own, buf, base

        def spot(self, half, sec, prim, low, count):
            zz, xx = (sec, prim) if half == 0 else (prim, sec)
            row = (zz * 4 + xx) * SHARD + half * HALF + low
            return self.buf.at[pl.ds(pl.multiple_of(row, 16), count)]

        def copy(self, half, index, src, dst, target):
            k = self.base + half * 20 + index
            return remote(src, dst, g_send.at[k], g_recv.at[k], target)

        def at(self, half):
            return (z, x) if half == 0 else (x, z)

        def towards(self, half, primary, by):
            if primary == (half == 0):
                return device(z, ring(x, by), y, c)
            return device(ring(z, by), x, y, c)

        def first(self):
            for half in (0, 1):
                sec, prim = self.at(half)
                src = self.own.at[pl.ds(half * HALF, HALF)]
                dst = self.spot(half, sec, prim, 0, HALF)
                for d, by in DIRS:
                    start(self.copy(half, d, src, dst, self.towards(half, True, by)))
            for half in (0, 1):
                sec, prim = self.at(half)
                src = self.own.at[pl.ds(half * HALF, HALF)]
                dst = self.spot(half, sec, prim, 0, HALF)
                for d, by in DIRS:
                    start(self.copy(half, 4 + d, src, dst, self.towards(half, False, by)))

        def wait(self, half, index, sec, prim, low, count):
            ref = self.spot(half, sec, prim, low, count)
            self.copy(half, index, ref, ref, partner).wait_recv()

        def second(self):
            for half in (0, 1):
                sec, prim = self.at(half)
                for d, by in DIRS:
                    origin = ring(prim, -by)
                    self.wait(half, d, sec, origin, 0, HALF)
                    piece = self.spot(half, sec, origin, d * QUARTER, QUARTER)
                    start(self.copy(half, 2 + d, piece, piece, self.towards(half, True, by)))
            for half in (0, 1):
                self.spread(half, 1)

        def spread(self, half, j):
            sec, prim = self.at(half)
            piece = self.spot(half, sec, ring(prim, STEPS[j]), 0, HALF)
            for d, by in DIRS:
                start(self.copy(half, 4 + 2 * j + d, piece, piece, self.towards(half, False, by)))

        def opposite(self, half):
            sec, prim = self.at(half)
            for d, by in DIRS:
                self.wait(half, 2 + d, sec, ring(prim, 2), d * QUARTER, QUARTER)

        def third(self):
            self.spread(0, 2)
            self.opposite(1)
            self.spread(1, 3)
            self.opposite(0)

        def fourth(self):
            self.spread(1, 2)
            self.spread(0, 3)

        def forward(self, k):
            for half in (0, 1):
                j = ORDER[half][k]
                sec, prim = self.at(half)
                origin = ring(prim, STEPS[j])
                for d, by in DIRS:
                    self.wait(half, 4 + 2 * j + d, ring(sec, -by), origin, 0, HALF)
                    piece = self.spot(half, ring(sec, -by), origin, d * QUARTER, QUARTER)
                    start(self.copy(half, 12 + 2 * j + d, piece, piece, self.towards(half, False, by)))

        def last(self, k):
            for half in (0, 1):
                j = ORDER[half][k]
                sec, prim = self.at(half)
                origin = ring(prim, STEPS[j])
                for d, by in DIRS:
                    self.wait(half, 12 + 2 * j + d, ring(sec, 2), origin, d * QUARTER, QUARTER)

    up_gather = Gather(up, up_all, 0)
    down_gather = Gather(down, down_all, 40)
    after = ((s + 1) % 16, t)
    tail = pl.ds(ROWS - WINDOW, WINDOW)
    halo_copies = [
        remote(keys.at[:, tail], halo_k, halo_send.at[0], halo_recv.at[0], after),
        remote(values.at[:, tail], halo_v, halo_send.at[1], halo_recv.at[1], after),
    ]
    for copy in halo_copies:
        start(copy)
    up_gather.first()

    def w_cols(yy, cc=0, count=FEATURES):
        return pl.ds(pl.multiple_of((yy * 2 + cc) * FEATURES, 128), count)

    def w_rows(yy, cc, low=0, count=HEADS):
        return w_all.at[pl.ds(pl.multiple_of((yy * 2 + cc) * HEADS + low, 32), count)]

    def w_relay(k, by):
        src = out_weight.at[pl.ds(k * HALF, HALF), w_cols(ring(y, 2), 0, 2 * FEATURES)]
        return remote(src, w_pass.at[k], w_send.at[5 + k], w_recv.at[5 + k], y_next[by])

    for k, by in DIRS:
        start(w_relay(k, by))
    start(remote(out_weight.at[:, w_cols(y, 1 - c)], w_rows(y, c), w_send.at[0], w_recv.at[0], partner))
    for k, by in DIRS:
        for cc in (0, 1):
            start(remote(
                out_weight.at[:, w_cols(ring(y, by), cc)], w_rows(y, c),
                w_send.at[1 + 2 * k + cc], w_recv.at[1 + 2 * k + c], (s, ring(y, by) * 2 + cc),
            ))

    def w_arrived(index, ref):
        remote(ref, ref, w_send.at[index], w_recv.at[index], partner).wait_recv()

    def w_pass_on():
        for k, by in DIRS:
            w_relay(k, by).wait_recv()
            for cc in (0, 1):
                start(remote(
                    w_pass.at[k, :, pl.ds(cc * FEATURES, FEATURES)], w_rows(ring(y, -by), c, k * HALF, HALF),
                    w_send.at[7 + 2 * k + cc], w_recv.at[7 + 2 * k + c], (s, ring(y, by) * 2 + cc),
                ))

    key_at = lax.broadcasted_iota(jnp.int32, (2 * WINDOW, 3 * WINDOW), 0)
    query_at = lax.broadcasted_iota(jnp.int32, (2 * WINDOW, 3 * WINDOW), 1) % WINDOW
    mine_row = t * HEADS

    def attend(n, key_band, value_band, allowed):
        lanes = pl.ds(pl.multiple_of(n * WINDOW, WINDOW), WINDOW)
        q = jnp.concatenate([q_v[pl.ds(g * HEAD_SIZE, HEAD_SIZE), lanes] for g in range(3)], axis=1)
        scores = dot(key_band, q, ((0,), (0,))) * HEAD_SIZE**-0.5
        masked = jnp.where(allowed, scores, -1e30)
        top = jnp.maximum(jnp.max(masked, axis=0, keepdims=True), sinks)
        powers = jnp.where(allowed, jnp.exp(masked - top), 0.0)
        denom = jnp.sum(powers, axis=0, keepdims=True) + jnp.exp(sinks - top)
        probs = (powers * (1.0 / denom)).astype(BF16)
        output = dot(value_band, probs, ((1,), (0,))).astype(BF16)
        for g in range(3):
            rows = pl.ds(pl.multiple_of(mine_row + g * HEAD_SIZE, HEAD_SIZE), HEAD_SIZE)
            att_all[rows, lanes] = output[:, g * WINDOW : (g + 1) * WINDOW]

    near = (key_at > query_at) & (key_at <= query_at + WINDOW)
    for copy in locals_[:4]:
        copy.wait()
    sinks = jnp.concatenate([jnp.full((1, WINDOW), sink[g], F32) for g in range(3)], axis=1)

    def attend_blocks(low, high):
        @pl.loop(low, high)
        def _(n):
            band = pl.ds(pl.multiple_of((n - 1) * WINDOW, WINDOW), 2 * WINDOW)
            attend(n, k_v[:, band], v_v[:, band], near)

    PART = ROWS // 2
    FIRST = (PART, 0)

    def att_rows(yy, cc, part, low=0, count=HEADS):
        row = (yy * 2 + cc) * HEADS + low
        return att_all.at[pl.ds(pl.multiple_of(row, 32), count), pl.ds(FIRST[part], PART)]

    def att_copy(part, index, ref, target):
        k = part * 8 + index
        return remote(ref, ref, att_send.at[k], att_recv.at[k], target)

    def att_arrived(part, index, ref):
        att_copy(part, index, ref, partner).wait_recv()

    def att_begin(part):
        for d, by in DIRS:
            start(att_copy(part, d, att_rows(y, c, part), y_next[by]))

    def att_pass(part):
        for d, by in DIRS:
            near_y = ring(y, -by)
            att_arrived(part, d, att_rows(near_y, c, part))
            start(att_copy(part, 2 + d, att_rows(near_y, c, part, d * HALF, HALF), y_next[by]))
            start(att_copy(part, 5 + d, att_rows(near_y, c, part), partner))

    def mix(yy, part, first):
        rows = pl.ds(pl.multiple_of(yy * 2 * HEADS, 2 * HEADS), 2 * HEADS)

        @pl.loop(0, PART // TILE)
        def _(i):
            tokens = pl.ds(pl.multiple_of(FIRST[part] + i * TILE, TILE), TILE)
            total = dot(att_all[rows, tokens], w_all[rows, :], ((0,), (0,)))
            mixed[tokens, :] = total if first else mixed[tokens, :] + total

    def mix_near(part):
        for d, by in DIRS:
            near_y = ring(y, -by)
            att_arrived(part, 5 + d, att_rows(near_y, 1 - c, part))
            if part == 0:
                for cc in (0, 1):
                    w_arrived(1 + 2 * d + cc, w_rows(near_y, cc))
            mix(near_y, part, False)

    def mix_far(part):
        far = ring(y, 2)
        for d, by in DIRS:
            att_arrived(part, 2 + d, att_rows(far, c, part, d * HALF, HALF))
        start(att_copy(part, 7, att_rows(far, c, part), partner))
        if part == 0:
            for d, by in DIRS:
                for cc in (0, 1):
                    w_arrived(7 + 2 * d + cc, w_rows(far, cc, d * HALF, HALF))
        att_arrived(part, 7, att_rows(far, 1 - c, part))
        mix(far, part, False)

    lanes_of = lambda cc: pl.ds(pl.multiple_of(cc * FEATURES, 128), FEATURES)

    def x_block(yy, cc, part, quarter=None):
        low, count = (0, PART) if quarter is None else (quarter * TILE, TILE)
        return x_all.at[pl.ds(pl.multiple_of(yy * ROWS + FIRST[part] + low, TILE), count), lanes_of(cc)]

    ones = jnp.ones((8, FEATURES), BF16)
    sq_rows = pl.ds(pl.multiple_of(t * 8, 8), 8)

    def make_x(part):
        gains = gain[...].astype(F32).reshape(1, FEATURES)

        @pl.loop(0, PART // TILE)
        def _(i):
            tokens = pl.ds(pl.multiple_of(FIRST[part] + i * TILE, TILE), TILE)
            here = (res_v[tokens, :].astype(F32) + mixed[tokens, :]).astype(BF16)
            stream[tokens, :] = here
            wide = here.astype(F32)
            rows = pl.ds(pl.multiple_of(y * ROWS + FIRST[part] + i * TILE, TILE), TILE)
            x_all[rows, lanes_of(c)] = (wide * gains).astype(BF16)
            sq = wide * wide
            high = sq.astype(BF16)
            low = (sq - high.astype(F32)).astype(BF16)
            squares[sq_rows, tokens] = dot(ones, high, ((1,), (1,))) + dot(ones, low, ((1,), (1,)))

    def x_copy(part, index, ref, target):
        k = part * 10 + index
        return remote(ref, ref, x_send.at[k], x_recv.at[k], target)

    def x_arrived(part, index, ref):
        x_copy(part, index, ref, partner).wait_recv()

    def x_begin(part, second):
        for d, by in DIRS:
            quarter = 1 - d if second else d
            start(x_copy(part, 2 * second + d, x_block(y, c, part, quarter), y_next[by]))

    def x_pass(part):
        for d, by in DIRS:
            ref = x_block(ring(y, -by), c, part, d)
            x_arrived(part, d, ref)
            start(x_copy(part, 4 + d, ref, y_next[by]))

    def x_near(part):
        for d, by in DIRS:
            x_arrived(part, 2 + d, x_block(ring(y, -by), c, part, 1 - d))
            start(x_copy(part, 7 + d, x_block(ring(y, -by), c, part), partner))

    def x_far(part):
        for d, by in DIRS:
            x_arrived(part, 4 + d, x_block(ring(y, 2), c, part, d))
        start(x_copy(part, 9, x_block(ring(y, 2), c, part), partner))

    def hide(yy, part, first=False, last=False):
        @pl.loop(0, PART // TILE)
        def _(i):
            tokens = pl.ds(pl.multiple_of(FIRST[part] + i * TILE, TILE), TILE)
            rows = pl.ds(pl.multiple_of(yy * ROWS + FIRST[part] + i * TILE, TILE), TILE)
            for n in range(3):
                cols = pl.ds(n * 512, 512)
                total = dot(x_all[rows, :], up_all[pl.ds(pl.multiple_of(yy * 768, 768), 768), cols], ((1,), (0,)))
                if not first:
                    total = total + hidden[tokens, cols]
                if last:
                    units = jnp.square(jnp.maximum(total, 0.0)).astype(BF16)
                    act_t[cols, tokens] = jnp.transpose(units)
                else:
                    hidden[tokens, cols] = total

    attend_blocks(4, 8)
    att_begin(0)
    start(att_copy(0, 4, att_rows(y, c, 0), partner))
    attend_blocks(1, 4)
    for copy in halo_copies:
        copy.wait_recv()
    first_key = jnp.where(s == 0, WINDOW, 0)
    attend(
        0,
        jnp.concatenate([halo_k[...], k_v[:, 0:WINDOW]], axis=1),
        jnp.concatenate([halo_v[...], v_v[:, 0:WINDOW]], axis=1),
        near & (key_at >= first_key),
    )
    start(att_copy(1, 4, att_rows(y, c, 1), partner))
    w_pass_on()
    up_gather.second()
    for copy in locals_[4:]:
        copy.wait()
    w_arrived(0, w_rows(y, 1 - c))
    for part in (0, 1):
        att_arrived(part, 4, att_rows(y, 1 - c, part))
        mix(y, part, True)
    att_pass(0)
    att_begin(1)
    up_gather.forward(0)
    up_gather.third()
    mix_near(0)
    mix_far(0)
    make_x(0)
    x_begin(0, False)
    att_pass(1)
    x_begin(0, True)
    start(x_copy(0, 6, x_block(y, c, 0), partner))
    up_gather.forward(1)
    up_gather.fourth()
    mix_near(1)
    x_pass(0)
    mix_far(1)
    make_x(1)
    x_begin(1, False)
    x_begin(1, True)
    start(x_copy(1, 6, x_block(y, c, 1), partner))
    sq_copies = []
    for k in range(1, 8):
        ref = squares.at[sq_rows]
        copy = remote(ref, ref, sq_send.at[k - 1], sq_recv.at[k - 1], (s, (t + k) % 8))
        start(copy)
        sq_copies.append(copy)
    x_near(0)
    up_gather.forward(2)
    x_far(0)
    up_gather.last(0)
    x_arrived(0, 6, x_block(y, 1 - c, 0))
    for d, by in DIRS:
        x_arrived(0, 7 + d, x_block(ring(y, -by), 1 - c, 0))
    x_arrived(0, 9, x_block(ring(y, 2), 1 - c, 0))
    hide(z, 0, first=True)
    up_gather.forward(3)
    down_gather.first()
    x_pass(1)
    up_gather.last(1)
    hide(ring(z, -1), 0)
    x_near(1)
    up_gather.last(2)
    up_gather.last(3)
    hide(ring(z, 1), 0)
    hide(ring(z, 2), 0, last=True)
    x_far(1)
    x_arrived(1, 6, x_block(y, 1 - c, 1))
    hide(y, 1, first=True)
    for d, by in DIRS:
        x_arrived(1, 7 + d, x_block(ring(y, -by), 1 - c, 1))
        hide(ring(y, -by), 1)
        if d == 0:
            down_gather.second()
    x_arrived(1, 9, x_block(ring(y, 2), 1 - c, 1))
    hide(ring(y, 2), 1, last=True)

    GROUPS = [[(half, 0, j) for j in range(3)] for half in (0, 1)]
    GROUPS.append([(half, 0, 3) for half in (0, 1)])
    for k in range(4):
        GROUPS.append([(half, i, ORDER[half][k]) for half in (0, 1) for i in (1, 2)])
        GROUPS.append([(half, 3, ORDER[half][k]) for half in (0, 1)])

    class Piece:
        def __init__(self, half, i, j):
            sec, prim = down_gather.at(half)
            sec, prim = ring(sec, STEPS[i]), ring(prim, STEPS[j])
            zz, xx = (sec, prim) if half == 0 else (prim, sec)
            self.row = (zz * 4 + xx) * SHARD + half * HALF
            self.half = half
            self.part = (xx % 2) * 2 + half
            self.mine = xx // 2 == c
            self.away = (y - zz + 4) % 4
            self.pair = zz * 4 + self.part

        def rows(self, low=0, count=HALF):
            return pl.ds(pl.multiple_of(self.row + low, 16), count)

        def paired_rows(self, low=0, count=HALF):
            return pl.ds(pl.multiple_of(self.pair * HALF + low, 16), count)

        def to_pair(self):
            return remote(
                partials.at[self.rows()], paired.at[self.paired_rows()],
                pair_send.at[self.pair], pair_recv.at[self.pair], partner,
            )

        def to_side(self):
            return remote(
                partials.at[self.rows()], chained.at[pl.ds(pl.multiple_of(self.part * HALF, 32), HALF)],
                side_send.at[self.part], side_recv.at[self.part], y_next[-1 if self.half == 0 else 1],
            )

        def to_owner(self):
            index = (self.away // 2) * 4 + self.part
            return remote(
                partials.at[self.rows()], final.at[pl.ds(pl.multiple_of(index * HALF, 32), HALF)],
                owner_send.at[index], owner_recv.at[index], (s, ring(y, -self.away) * 2 + c),
            )

        def add(self, side):
            for k in (0, 1):
                rows = self.rows(k * QUARTER, QUARTER)
                total = partials[rows, :].astype(F32) + paired[self.paired_rows(k * QUARTER, QUARTER), :].astype(F32)
                if side:
                    there = pl.ds(pl.multiple_of(self.part * HALF + k * QUARTER, 16), QUARTER)
                    total = total + chained[there, :].astype(F32)
                partials[rows, :] = total.astype(BF16)

    groups = [[Piece(*facts) for facts in group] for group in GROUPS]

    def compute(group):
        @pl.loop(0, ROWS // TILE)
        def _(i):
            tokens = pl.ds(pl.multiple_of(i * TILE, TILE), TILE)
            weight = jnp.concatenate([down_all[p.rows(), :] for p in group], axis=0)
            part = dot(weight, act_t[:, tokens], ((1,), (0,))).astype(BF16)
            for k, p in enumerate(group):
                partials[p.rows(), tokens] = part[k * HALF : (k + 1) * HALF]

        for p in group:
            @pl.when(jnp.logical_not(p.mine))
            def _():
                p.to_pair().start()

    def combine(group):
        for p in group:
            side = 1 if p.half == 0 else 3

            @pl.when(p.mine & (p.away != 0) & (p.away != side))
            def _():
                p.to_pair().wait_recv()
                p.add(False)

                @pl.when(p.away == 2)
                def _():
                    p.to_side().start()

                @pl.when(p.away != 2)
                def _():
                    p.to_owner().start()

    def relay(group):
        for p in group:
            @pl.when(p.mine & (p.away == (1 if p.half == 0 else 3)))
            def _():
                p.to_pair().wait_recv()
                p.to_side().wait_recv()
                p.add(True)
                p.to_owner().start()

    compute(groups[0])
    compute(groups[1])
    combine(groups[0])
    down_gather.forward(0)
    compute(groups[3])
    combine(groups[1])
    down_gather.third()
    compute(groups[2])
    combine(groups[3])
    combine(groups[2])
    down_gather.forward(1)
    down_gather.fourth()
    compute(groups[5])
    relay(groups[0])
    relay(groups[1])
    down_gather.last(0)
    combine(groups[5])
    compute(groups[4])
    combine(groups[4])
    relay(groups[3])
    down_gather.forward(2)
    compute(groups[7])
    relay(groups[2])
    combine(groups[7])
    down_gather.last(1)
    compute(groups[6])
    combine(groups[6])
    relay(groups[5])
    relay(groups[4])
    down_gather.forward(3)
    compute(groups[9])
    combine(groups[9])
    relay(groups[7])
    down_gather.last(2)
    compute(groups[8])
    combine(groups[8])
    relay(groups[6])
    down_gather.last(3)
    compute(groups[10])
    combine(groups[10])
    relay(groups[9])
    relay(groups[8])
    relay(groups[10])

    for copy in sq_copies:
        copy.wait_recv()
    own = [Piece(half, 0, 0) for half in (0, 1, 0, 1)]
    for part, p in enumerate(own):
        p.part = part
        p.half = part % 2
        p.row = (y * 4 + c * 2) * SHARD + part * HALF
        p.pair = y * 4 + part
    for p in own:
        p.to_pair().wait_recv()
        for away in (1, 3):
            p.away = away
            p.to_owner().wait_recv()
    mine = pl.ds(pl.multiple_of((y * 4 + c * 2) * SHARD, FEATURES), FEATURES)
    beside = pl.ds(pl.multiple_of(y * FEATURES, FEATURES), FEATURES)

    @pl.loop(0, ROWS // 128)
    def _(i):
        tokens = pl.ds(pl.multiple_of(i * 128, 128), 128)
        total = partials[mine, tokens].astype(F32) + paired[beside, tokens].astype(F32)
        for k in range(2):
            total = total + final[k * FEATURES : (k + 1) * FEATURES, tokens].astype(F32)
        norm = squares[0:1, tokens]
        for k in range(1, 8):
            norm = norm + squares[8 * k : 8 * k + 1, tokens]
        total = total * (1.0 / (norm * (1.0 / D) + EPSILON))
        result[tokens, :] = (stream[tokens, :].astype(F32) + jnp.transpose(total)).astype(BF16)

    for copy in pending:
        copy.wait_send()
    for k in range(16):
        p = own[0]
        p.pair = k
        p.to_pair().wait_send()
    for p in own:
        p.to_side().wait_send()
        for away in (1, 3):
            p.away = away
            p.to_owner().wait_send()


def body(
    queries, key_heads, projected_value_heads, sink_logit_table, out_weight,
    residual, norm_gain, up_weight, down_weight,
):
    hbm = pl.BlockSpec(memory_space=pl.ANY)
    dma = pltpu.SemaphoreType.DMA
    return pl.pallas_call(
        kernel,
        out_shape=pltpu.VMEM((ROWS, FEATURES), BF16),
        in_specs=[hbm] * 9,
        out_specs=pl.BlockSpec(memory_space=pltpu.VMEM),
        scratch_shapes=[
            pltpu.VMEM((D, HIDDEN), BF16),
            pltpu.VMEM((D, HIDDEN), BF16),
            pltpu.VMEM((4 * ROWS, 2 * FEATURES), BF16),
            pltpu.VMEM((8 * HEADS, ROWS), BF16),
            pltpu.VMEM((8 * HEADS, FEATURES), BF16),
            pltpu.VMEM((2, HALF, 2 * FEATURES), BF16),
            pltpu.VMEM((ROWS, HIDDEN), F32),
            pltpu.VMEM((HIDDEN, ROWS), BF16),
            pltpu.VMEM((ROWS, FEATURES), F32),
            pltpu.VMEM((ROWS, FEATURES), BF16),
            pltpu.VMEM((ROWS, FEATURES), BF16),
            pltpu.VMEM((HEADS, ROWS), BF16),
            pltpu.VMEM((HEAD_SIZE, ROWS), BF16),
            pltpu.VMEM((HEAD_SIZE, ROWS), BF16),
            pltpu.VMEM((HEAD_SIZE, WINDOW), BF16),
            pltpu.VMEM((HEAD_SIZE, WINDOW), BF16),
            pltpu.VMEM((D, ROWS), BF16),
            pltpu.VMEM((D // 2, ROWS), BF16),
            pltpu.VMEM((FEATURES, ROWS), BF16),
            pltpu.VMEM((2 * FEATURES, ROWS), BF16),
            pltpu.VMEM((64, ROWS), F32),
            pltpu.SMEM((3,), F32),
            pltpu.VMEM((FEATURES,), BF16),
            dma((9,)), dma((11,)), dma((11,)), dma((2,)), dma((2,)), dma((80,)), dma((80,)),
            dma((16,)), dma((16,)), dma((20,)), dma((20,)), dma((7,)), dma((7,)),
            dma((16,)), dma((16,)), dma((4,)), dma((4,)), dma((8,)), dma((8,)),
        ],
        compiler_params=pltpu.CompilerParams(
            collective_id=0, has_side_effects=True, vmem_limit_bytes=60 * 2**20
        ),
    )(
        queries.T, key_heads.T, projected_value_heads.T, sink_logit_table, out_weight,
        residual, norm_gain, up_weight, down_weight.T,
    )


def solution(mesh):
    return jax.shard_map(
        body,
        mesh=mesh,
        in_specs=(
            P("sp", "tp"), P("sp", "tp"), P("sp", "tp"), P("tp"), P("tp", None),
            P("sp", "tp"), P("tp"), P("sp", "tp"), P("tp", "sp"),
        ),
        out_specs=P("sp", "tp"),
        check_vma=False,
    )
```

```python
import functools

import jax
import jax.numpy as jnp
from jax import lax
from jax.experimental import pallas as pl
from jax.experimental.pallas import tpu as pltpu
from jax.sharding import PartitionSpec as P

D = 3072
HEAD_SIZE = 64
WINDOW = 128
EPSILON = 1e-06

ROWS = 1024
FEATURES = 384
HEADS = 192
SHARD = 192
HALF = 96
QUARTER = 48
HIDDEN = 1536
TILE = 256

MESH = pl.DeviceIdType.MESH
BF16 = jnp.bfloat16
F32 = jnp.float32


def dot(a, b, dims):
    return lax.dot_general(a, b, (dims, ((), ())), preferred_element_type=F32)


def kernel(
    queries, keys, values, sinks_in, out_weight, residual, gains_in, up, down,
    result,
    up_all, down_all, x_all, att_all, w_all, w_pass, hidden, act_t, mixed, stream, res_v,
    q_v, k_v, v_v, halo_k, halo_v, partials, paired, chained, final, squares, sink, gain,
    local_sem, w_send, w_recv, halo_send, halo_recv, g_send, g_recv,
    att_send, att_recv, x_send, x_recv, sq_send, sq_recv,
    pair_send, pair_recv, side_send, side_recv, owner_send, owner_recv,
):
    s, t = lax.axis_index("sp"), lax.axis_index("tp")
    z, x = s // 4, s % 4
    y, c = t // 2, t % 2

    def ring(position, by):
        return (position + by + 4) % 4

    def device(zz, xx, yy, cc):
        return (zz * 4 + xx, yy * 2 + cc)

    partner = (s, y * 2 + (1 - c))
    y_next = {1: (s, ring(y, 1) * 2 + c), -1: (s, ring(y, -1) * 2 + c)}
    DIRS = ((0, 1), (1, -1))

    def remote(src, dst, send, recv, target):
        return pltpu.make_async_remote_copy(
            src_ref=src, dst_ref=dst, send_sem=send, recv_sem=recv,
            device_id=target, device_id_type=MESH,
        )

    pending = []

    def start(copy):
        copy.start()
        pending.append(copy)

    barrier = pltpu.get_barrier_semaphore()
    greeted = [
        device(z, ring(x, 1), y, c), device(z, ring(x, -1), y, c),
        device(ring(z, 1), x, y, c), device(ring(z, -1), x, y, c),
        ((s + 1) % 16, t), ((s + 15) % 16, t),
    ] + [(s, (t + k) % 8) for k in range(1, 8)]
    for other in greeted:
        pl.semaphore_signal(barrier, inc=1, device_id=other, device_id_type=MESH)
    locals_ = [
        pltpu.make_async_copy(src, dst, local_sem.at[i])
        for i, (src, dst) in enumerate([
            (queries, q_v), (keys, k_v), (values, v_v), (sinks_in, sink), (gains_in, gain), (residual, res_v),
            (up, up_all.at[pl.ds(pl.multiple_of(s * SHARD, SHARD), SHARD)]),
            (down, down_all.at[pl.ds(pl.multiple_of(s * SHARD, SHARD), SHARD)]),
            (out_weight.at[:, pl.ds(pl.multiple_of(t * FEATURES, 128), FEATURES)],
             w_all.at[pl.ds(pl.multiple_of(t * HEADS, HEADS), HEADS)]),
        ])
    ]
    for copy in locals_:
        copy.start()
    pl.semaphore_wait(barrier, len(greeted))

    STEPS = (0, -1, 1, 2)
    ORDER = ((0, 1, 2, 3), (0, 1, 3, 2))

    class Gather:
        def __init__(self, own, buf, base):
            self.own, self.buf, self.base = own, buf, base

        def spot(self, half, sec, prim, low, count):
            zz, xx = (sec, prim) if half == 0 else (prim, sec)
            row = (zz * 4 + xx) * SHARD + half * HALF + low
            return self.buf.at[pl.ds(pl.multiple_of(row, 16), count)]

        def copy(self, half, index, src, dst, target):
            k = self.base + half * 20 + index
            return remote(src, dst, g_send.at[k], g_recv.at[k], target)

        def at(self, half):
            return (z, x) if half == 0 else (x, z)

        def towards(self, half, primary, by):
            if primary == (half == 0):
                return device(z, ring(x, by), y, c)
            return device(ring(z, by), x, y, c)

        def first(self):
            for half in (0, 1):
                sec, prim = self.at(half)
                src = self.own.at[pl.ds(half * HALF, HALF)]
                dst = self.spot(half, sec, prim, 0, HALF)
                for d, by in DIRS:
                    start(self.copy(half, d, src, dst, self.towards(half, True, by)))
            for half in (0, 1):
                sec, prim = self.at(half)
                src = self.own.at[pl.ds(half * HALF, HALF)]
                dst = self.spot(half, sec, prim, 0, HALF)
                for d, by in DIRS:
                    start(self.copy(half, 4 + d, src, dst, self.towards(half, False, by)))

        def wait(self, half, index, sec, prim, low, count):
            ref = self.spot(half, sec, prim, low, count)
            self.copy(half, index, ref, ref, partner).wait_recv()

        def second(self):
            for half in (0, 1):
                sec, prim = self.at(half)
                for d, by in DIRS:
                    origin = ring(prim, -by)
                    self.wait(half, d, sec, origin, 0, HALF)
                    piece = self.spot(half, sec, origin, d * QUARTER, QUARTER)
                    start(self.copy(half, 2 + d, piece, piece, self.towards(half, True, by)))
            for half in (0, 1):
                self.spread(half, 1)

        def spread(self, half, j):
            sec, prim = self.at(half)
            piece = self.spot(half, sec, ring(prim, STEPS[j]), 0, HALF)
            for d, by in DIRS:
                start(self.copy(half, 4 + 2 * j + d, piece, piece, self.towards(half, False, by)))

        def opposite(self, half):
            sec, prim = self.at(half)
            for d, by in DIRS:
                self.wait(half, 2 + d, sec, ring(prim, 2), d * QUARTER, QUARTER)

        def third(self):
            self.spread(0, 2)
            self.opposite(1)
            self.spread(1, 3)
            self.opposite(0)

        def fourth(self):
            self.spread(1, 2)
            self.spread(0, 3)

        def forward(self, k):
            for half in (0, 1):
                j = ORDER[half][k]
                sec, prim = self.at(half)
                origin = ring(prim, STEPS[j])
                for d, by in DIRS:
                    self.wait(half, 4 + 2 * j + d, ring(sec, -by), origin, 0, HALF)
                    piece = self.spot(half, ring(sec, -by), origin, d * QUARTER, QUARTER)
                    start(self.copy(half, 12 + 2 * j + d, piece, piece, self.towards(half, False, by)))

        def last(self, k):
            for half in (0, 1):
                j = ORDER[half][k]
                sec, prim = self.at(half)
                origin = ring(prim, STEPS[j])
                for d, by in DIRS:
                    self.wait(half, 12 + 2 * j + d, ring(sec, 2), origin, d * QUARTER, QUARTER)

    up_gather = Gather(up, up_all, 0)
    down_gather = Gather(down, down_all, 40)
    after = ((s + 1) % 16, t)
    tail = pl.ds(ROWS - WINDOW, WINDOW)
    halo_copies = [
        remote(keys.at[:, tail], halo_k, halo_send.at[0], halo_recv.at[0], after),
        remote(values.at[:, tail], halo_v, halo_send.at[1], halo_recv.at[1], after),
    ]
    for copy in halo_copies:
        start(copy)
    up_gather.first()

    def w_cols(yy, cc=0, count=FEATURES):
        return pl.ds(pl.multiple_of((yy * 2 + cc) * FEATURES, 128), count)

    def w_rows(yy, cc, low=0, count=HEADS):
        return w_all.at[pl.ds(pl.multiple_of((yy * 2 + cc) * HEADS + low, 32), count)]

    def w_relay(k, by):
        src = out_weight.at[pl.ds(k * HALF, HALF), w_cols(ring(y, 2), 0, 2 * FEATURES)]
        return remote(src, w_pass.at[k], w_send.at[5 + k], w_recv.at[5 + k], y_next[by])

    for k, by in DIRS:
        start(w_relay(k, by))
    start(remote(out_weight.at[:, w_cols(y, 1 - c)], w_rows(y, c), w_send.at[0], w_recv.at[0], partner))
    for k, by in DIRS:
        for cc in (0, 1):
            start(remote(
                out_weight.at[:, w_cols(ring(y, by), cc)], w_rows(y, c),
                w_send.at[1 + 2 * k + cc], w_recv.at[1 + 2 * k + c], (s, ring(y, by) * 2 + cc),
            ))

    def w_arrived(index, ref):
        remote(ref, ref, w_send.at[index], w_recv.at[index], partner).wait_recv()

    def w_pass_on():
        for k, by in DIRS:
            w_relay(k, by).wait_recv()
            for cc in (0, 1):
                start(remote(
                    w_pass.at[k, :, pl.ds(cc * FEATURES, FEATURES)], w_rows(ring(y, -by), c, k * HALF, HALF),
                    w_send.at[7 + 2 * k + cc], w_recv.at[7 + 2 * k + c], (s, ring(y, by) * 2 + cc),
                ))

    key_at = lax.broadcasted_iota(jnp.int32, (2 * WINDOW, 3 * WINDOW), 0)
    query_at = lax.broadcasted_iota(jnp.int32, (2 * WINDOW, 3 * WINDOW), 1) % WINDOW
    mine_row = t * HEADS

    def attend(n, key_band, value_band, allowed):
        lanes = pl.ds(pl.multiple_of(n * WINDOW, WINDOW), WINDOW)
        q = jnp.concatenate([q_v[pl.ds(g * HEAD_SIZE, HEAD_SIZE), lanes] for g in range(3)], axis=1)
        scores = dot(key_band, q, ((0,), (0,))) * HEAD_SIZE**-0.5
        masked = jnp.where(allowed, scores, -1e30)
        top = jnp.maximum(jnp.max(masked, axis=0, keepdims=True), sinks)
        powers = jnp.where(allowed, jnp.exp(masked - top), 0.0)
        denom = jnp.sum(powers, axis=0, keepdims=True) + jnp.exp(sinks - top)
        probs = (powers * (1.0 / denom)).astype(BF16)
        output = dot(value_band, probs, ((1,), (0,))).astype(BF16)
        for g in range(3):
            rows = pl.ds(pl.multiple_of(mine_row + g * HEAD_SIZE, HEAD_SIZE), HEAD_SIZE)
            att_all[rows, lanes] = output[:, g * WINDOW : (g + 1) * WINDOW]

    near = (key_at > query_at) & (key_at <= query_at + WINDOW)
    for copy in locals_[:4]:
        copy.wait()
    sinks = jnp.concatenate([jnp.full((1, WINDOW), sink[g], F32) for g in range(3)], axis=1)

    def attend_blocks(low, high):
        @pl.loop(low, high)
        def _(n):
            band = pl.ds(pl.multiple_of((n - 1) * WINDOW, WINDOW), 2 * WINDOW)
            attend(n, k_v[:, band], v_v[:, band], near)

    PART = ROWS // 2
    FIRST = (PART, 0)

    def att_rows(yy, cc, part, low=0, count=HEADS):
        row = (yy * 2 + cc) * HEADS + low
        return att_all.at[pl.ds(pl.multiple_of(row, 32), count), pl.ds(FIRST[part], PART)]

    def att_copy(part, index, ref, target):
        k = part * 8 + index
        return remote(ref, ref, att_send.at[k], att_recv.at[k], target)

    def att_arrived(part, index, ref):
        att_copy(part, index, ref, partner).wait_recv()

    def att_begin(part):
        for d, by in DIRS:
            start(att_copy(part, d, att_rows(y, c, part), y_next[by]))

    def att_pass(part):
        for d, by in DIRS:
            near_y = ring(y, -by)
            att_arrived(part, d, att_rows(near_y, c, part))
            start(att_copy(part, 2 + d, att_rows(near_y, c, part, d * HALF, HALF), y_next[by]))
            start(att_copy(part, 5 + d, att_rows(near_y, c, part), partner))

    def mix(yy, part, first):
        rows = pl.ds(pl.multiple_of(yy * 2 * HEADS, 2 * HEADS), 2 * HEADS)

        @pl.loop(0, PART // TILE)
        def _(i):
            tokens = pl.ds(pl.multiple_of(FIRST[part] + i * TILE, TILE), TILE)
            total = dot(att_all[rows, tokens], w_all[rows, :], ((0,), (0,)))
            mixed[tokens, :] = total if first else mixed[tokens, :] + total

    def mix_near(part):
        for d, by in DIRS:
            near_y = ring(y, -by)
            att_arrived(part, 5 + d, att_rows(near_y, 1 - c, part))
            if part == 0:
                for cc in (0, 1):
                    w_arrived(1 + 2 * d + cc, w_rows(near_y, cc))
            mix(near_y, part, False)

    def mix_far(part):
        far = ring(y, 2)
        for d, by in DIRS:
            att_arrived(part, 2 + d, att_rows(far, c, part, d * HALF, HALF))
        start(att_copy(part, 7, att_rows(far, c, part), partner))
        if part == 0:
            for d, by in DIRS:
                for cc in (0, 1):
                    w_arrived(7 + 2 * d + cc, w_rows(far, cc, d * HALF, HALF))
        att_arrived(part, 7, att_rows(far, 1 - c, part))
        mix(far, part, False)

    lanes_of = lambda cc: pl.ds(pl.multiple_of(cc * FEATURES, 128), FEATURES)

    def x_block(yy, cc, part, quarter=None):
        low, count = (0, PART) if quarter is None else (quarter * TILE, TILE)
        return x_all.at[pl.ds(pl.multiple_of(yy * ROWS + FIRST[part] + low, TILE), count), lanes_of(cc)]

    ones = jnp.ones((8, FEATURES), BF16)
    sq_rows = pl.ds(pl.multiple_of(t * 8, 8), 8)

    def make_x(part):
        gains = gain[...].astype(F32).reshape(1, FEATURES)

        @pl.loop(0, PART // TILE)
        def _(i):
            tokens = pl.ds(pl.multiple_of(FIRST[part] + i * TILE, TILE), TILE)
            here = (res_v[tokens, :].astype(F32) + mixed[tokens, :]).astype(BF16)
            stream[tokens, :] = here
            wide = here.astype(F32)
            rows = pl.ds(pl.multiple_of(y * ROWS + FIRST[part] + i * TILE, TILE), TILE)
            x_all[rows, lanes_of(c)] = (wide * gains).astype(BF16)
            sq = wide * wide
            high = sq.astype(BF16)
            low = (sq - high.astype(F32)).astype(BF16)
            squares[sq_rows, tokens] = dot(ones, high, ((1,), (1,))) + dot(ones, low, ((1,), (1,)))

    def x_copy(part, index, ref, target):
        k = part * 10 + index
        return remote(ref, ref, x_send.at[k], x_recv.at[k], target)

    def x_arrived(part, index, ref):
        x_copy(part, index, ref, partner).wait_recv()

    def x_begin(part, second):
        for d, by in DIRS:
            quarter = 1 - d if second else d
            start(x_copy(part, 2 * second + d, x_block(y, c, part, quarter), y_next[by]))

    def x_pass(part):
        for d, by in DIRS:
            ref = x_block(ring(y, -by), c, part, d)
            x_arrived(part, d, ref)
            start(x_copy(part, 4 + d, ref, y_next[by]))

    def x_near(part):
        for d, by in DIRS:
            x_arrived(part, 2 + d, x_block(ring(y, -by), c, part, 1 - d))
            start(x_copy(part, 7 + d, x_block(ring(y, -by), c, part), partner))

    def x_far(part):
        for d, by in DIRS:
            x_arrived(part, 4 + d, x_block(ring(y, 2), c, part, d))
        start(x_copy(part, 9, x_block(ring(y, 2), c, part), partner))

    def hide(yy, part, first=False, last=False):
        @pl.loop(0, PART // TILE)
        def _(i):
            tokens = pl.ds(pl.multiple_of(FIRST[part] + i * TILE, TILE), TILE)
            rows = pl.ds(pl.multiple_of(yy * ROWS + FIRST[part] + i * TILE, TILE), TILE)
            for n in range(3):
                cols = pl.ds(n * 512, 512)
                total = dot(x_all[rows, :], up_all[pl.ds(pl.multiple_of(yy * 768, 768), 768), cols], ((1,), (0,)))
                if not first:
                    total = total + hidden[tokens, cols]
                if last:
                    units = jnp.square(jnp.maximum(total, 0.0)).astype(BF16)
                    act_t[cols, tokens] = jnp.transpose(units)
                else:
                    hidden[tokens, cols] = total

    attend_blocks(4, 8)
    att_begin(0)
    start(att_copy(0, 4, att_rows(y, c, 0), partner))
    attend_blocks(1, 4)
    for copy in halo_copies:
        copy.wait_recv()
    first_key = jnp.where(s == 0, WINDOW, 0)
    attend(
        0,
        jnp.concatenate([halo_k[...], k_v[:, 0:WINDOW]], axis=1),
        jnp.concatenate([halo_v[...], v_v[:, 0:WINDOW]], axis=1),
        near & (key_at >= first_key),
    )
    start(att_copy(1, 4, att_rows(y, c, 1), partner))
    w_pass_on()
    up_gather.second()
    for copy in locals_[4:]:
        copy.wait()
    w_arrived(0, w_rows(y, 1 - c))
    for part in (0, 1):
        att_arrived(part, 4, att_rows(y, 1 - c, part))
        mix(y, part, True)
    att_pass(0)
    att_begin(1)
    up_gather.forward(0)
    up_gather.third()
    mix_near(0)
    mix_far(0)
    make_x(0)
    x_begin(0, False)
    att_pass(1)
    x_begin(0, True)
    start(x_copy(0, 6, x_block(y, c, 0), partner))
    up_gather.forward(1)
    up_gather.fourth()
    mix_near(1)
    x_pass(0)
    mix_far(1)
    make_x(1)
    x_begin(1, False)
    x_begin(1, True)
    start(x_copy(1, 6, x_block(y, c, 1), partner))
    sq_copies = []
    for k in range(1, 8):
        ref = squares.at[sq_rows]
        copy = remote(ref, ref, sq_send.at[k - 1], sq_recv.at[k - 1], (s, (t + k) % 8))
        start(copy)
        sq_copies.append(copy)
    x_near(0)
    up_gather.forward(2)
    x_far(0)
    up_gather.last(0)
    x_arrived(0, 6, x_block(y, 1 - c, 0))
    for d, by in DIRS:
        x_arrived(0, 7 + d, x_block(ring(y, -by), 1 - c, 0))
    x_arrived(0, 9, x_block(ring(y, 2), 1 - c, 0))
    hide(z, 0, first=True)
    up_gather.forward(3)
    down_gather.first()
    x_pass(1)
    up_gather.last(1)
    hide(ring(z, -1), 0)
    x_near(1)
    up_gather.last(2)
    up_gather.last(3)
    hide(ring(z, 1), 0)
    hide(ring(z, 2), 0, last=True)
    x_far(1)
    x_arrived(1, 6, x_block(y, 1 - c, 1))
    hide(y, 1, first=True)
    for d, by in DIRS:
        x_arrived(1, 7 + d, x_block(ring(y, -by), 1 - c, 1))
        hide(ring(y, -by), 1)
        if d == 0:
            down_gather.second()
    x_arrived(1, 9, x_block(ring(y, 2), 1 - c, 1))
    hide(ring(y, 2), 1, last=True)

    GROUPS = [[(half, 0, j) for j in range(3)] for half in (0, 1)]
    GROUPS.append([(half, 0, 3) for half in (0, 1)])
    for k in range(4):
        GROUPS.append([(half, i, ORDER[half][k]) for half in (0, 1) for i in (1, 2)])
        GROUPS.append([(half, 3, ORDER[half][k]) for half in (0, 1)])

    def lanes(part):
        return pl.ds(pl.multiple_of(part * PART, PART), PART)

    class Piece:
        def __init__(self, half, i, j):
            sec, prim = down_gather.at(half)
            sec, prim = ring(sec, STEPS[i]), ring(prim, STEPS[j])
            zz, xx = (sec, prim) if half == 0 else (prim, sec)
            self.row = (zz * 4 + xx) * SHARD + half * HALF
            self.half = half
            self.part = (xx % 2) * 2 + half
            self.mine = xx // 2 == c
            self.away = (y - zz + 4) % 4
            self.pair = zz * 4 + self.part

        def rows(self, low=0, count=HALF):
            return pl.ds(pl.multiple_of(self.row + low, 16), count)

        def paired_rows(self, low=0, count=HALF):
            return pl.ds(pl.multiple_of(self.pair * HALF + low, 16), count)

        def to_pair(self, part):
            k = self.pair * 2 + part
            return remote(
                partials.at[self.rows(), lanes(part)], paired.at[self.paired_rows(), lanes(part)],
                pair_send.at[k], pair_recv.at[k], partner,
            )

        def to_side(self, part):
            k = self.part * 2 + part
            return remote(
                partials.at[self.rows(), lanes(part)],
                chained.at[pl.ds(pl.multiple_of(self.part * HALF, 32), HALF), lanes(part)],
                side_send.at[k], side_recv.at[k], y_next[-1 if self.half == 0 else 1],
            )

        def to_owner(self, part):
            index = (self.away // 2) * 4 + self.part
            k = index * 2 + part
            return remote(
                partials.at[self.rows(), lanes(part)],
                final.at[pl.ds(pl.multiple_of(index * HALF, 32), HALF), lanes(part)],
                owner_send.at[k], owner_recv.at[k], (s, ring(y, -self.away) * 2 + c),
            )

        def add(self, part, side):
            rows = self.rows()
            total = partials[rows, lanes(part)].astype(F32) + paired[self.paired_rows(), lanes(part)].astype(F32)
            if side:
                there = pl.ds(pl.multiple_of(self.part * HALF, 32), HALF)
                total = total + chained[there, lanes(part)].astype(F32)
            partials[rows, lanes(part)] = total.astype(BF16)

    groups = [[Piece(*facts) for facts in group] for group in GROUPS]

    def compute(group):
        @pl.loop(0, 2)
        def _(part):
            @pl.loop(0, PART // TILE)
            def _(i):
                tokens = pl.ds(pl.multiple_of(part * PART + i * TILE, TILE), TILE)
                weight = jnp.concatenate([down_all[p.rows(), :] for p in group], axis=0)
                total = dot(weight, act_t[:, tokens], ((1,), (0,))).astype(BF16)
                for k, p in enumerate(group):
                    partials[p.rows(), tokens] = total[k * HALF : (k + 1) * HALF]

            for p in group:
                @pl.when(jnp.logical_not(p.mine))
                def _():
                    p.to_pair(part).start()

    def combine(group):
        @pl.loop(0, 2)
        def _(part):
            for p in group:
                side = 1 if p.half == 0 else 3

                @pl.when(p.mine & (p.away != 0) & (p.away != side))
                def _():
                    p.to_pair(part).wait_recv()
                    p.add(part, False)

                    @pl.when(p.away == 2)
                    def _():
                        p.to_side(part).start()

                    @pl.when(p.away != 2)
                    def _():
                        p.to_owner(part).start()

    def relay(group):
        @pl.loop(0, 2)
        def _(part):
            for p in group:
                @pl.when(p.mine & (p.away == (1 if p.half == 0 else 3)))
                def _():
                    p.to_pair(part).wait_recv()
                    p.to_side(part).wait_recv()
                    p.add(part, True)
                    p.to_owner(part).start()

    compute(groups[0])
    compute(groups[1])
    combine(groups[0])
    down_gather.forward(0)
    compute(groups[3])
    combine(groups[1])
    down_gather.third()
    compute(groups[2])
    combine(groups[3])
    combine(groups[2])
    down_gather.forward(1)
    down_gather.fourth()
    compute(groups[5])
    relay(groups[0])
    relay(groups[1])
    down_gather.last(0)
    combine(groups[5])
    compute(groups[4])
    combine(groups[4])
    relay(groups[3])
    down_gather.forward(2)
    compute(groups[7])
    relay(groups[2])
    combine(groups[7])
    down_gather.last(1)
    compute(groups[6])
    combine(groups[6])
    relay(groups[5])
    relay(groups[4])
    down_gather.forward(3)
    compute(groups[9])
    combine(groups[9])
    relay(groups[7])
    down_gather.last(2)
    compute(groups[8])
    combine(groups[8])
    relay(groups[6])
    down_gather.last(3)
    compute(groups[10])
    combine(groups[10])
    relay(groups[9])
    relay(groups[8])
    relay(groups[10])

    for copy in sq_copies:
        copy.wait_recv()
    own = [Piece(half, 0, 0) for half in (0, 1, 0, 1)]
    for part, p in enumerate(own):
        p.part = part
        p.half = part % 2
        p.row = (y * 4 + c * 2) * SHARD + part * HALF
        p.pair = y * 4 + part
    mine = pl.ds(pl.multiple_of((y * 4 + c * 2) * SHARD, FEATURES), FEATURES)
    beside = pl.ds(pl.multiple_of(y * FEATURES, FEATURES), FEATURES)

    @pl.loop(0, 2)
    def _(part):
        for p in own:
            p.to_pair(part).wait_recv()
            for away in (1, 3):
                p.away = away
                p.to_owner(part).wait_recv()

        @pl.loop(0, PART // 128)
        def _(i):
            tokens = pl.ds(pl.multiple_of(part * PART + i * 128, 128), 128)
            total = partials[mine, tokens].astype(F32) + paired[beside, tokens].astype(F32)
            for k in range(2):
                total = total + final[k * FEATURES : (k + 1) * FEATURES, tokens].astype(F32)
            norm = squares[0:1, tokens]
            for k in range(1, 8):
                norm = norm + squares[8 * k : 8 * k + 1, tokens]
            total = total * (1.0 / (norm * (1.0 / D) + EPSILON))
            result[tokens, :] = (stream[tokens, :].astype(F32) + jnp.transpose(total)).astype(BF16)

    for copy in pending:
        copy.wait_send()
    for part in (0, 1):
        for k in range(16):
            p = own[0]
            p.pair = k
            p.to_pair(part).wait_send()
        for p in own:
            p.to_side(part).wait_send()
            for away in (1, 3):
                p.away = away
                p.to_owner(part).wait_send()


def body(
    queries, key_heads, projected_value_heads, sink_logit_table, out_weight,
    residual, norm_gain, up_weight, down_weight,
):
    hbm = pl.BlockSpec(memory_space=pl.ANY)
    dma = pltpu.SemaphoreType.DMA
    return pl.pallas_call(
        kernel,
        out_shape=pltpu.VMEM((ROWS, FEATURES), BF16),
        in_specs=[hbm] * 9,
        out_specs=pl.BlockSpec(memory_space=pltpu.VMEM),
        scratch_shapes=[
            pltpu.VMEM((D, HIDDEN), BF16),
            pltpu.VMEM((D, HIDDEN), BF16),
            pltpu.VMEM((4 * ROWS, 2 * FEATURES), BF16),
            pltpu.VMEM((8 * HEADS, ROWS), BF16),
            pltpu.VMEM((8 * HEADS, FEATURES), BF16),
            pltpu.VMEM((2, HALF, 2 * FEATURES), BF16),
            pltpu.VMEM((ROWS, HIDDEN), F32),
            pltpu.VMEM((HIDDEN, ROWS), BF16),
            pltpu.VMEM((ROWS, FEATURES), F32),
            pltpu.VMEM((ROWS, FEATURES), BF16),
            pltpu.VMEM((ROWS, FEATURES), BF16),
            pltpu.VMEM((HEADS, ROWS), BF16),
            pltpu.VMEM((HEAD_SIZE, ROWS), BF16),
            pltpu.VMEM((HEAD_SIZE, ROWS), BF16),
            pltpu.VMEM((HEAD_SIZE, WINDOW), BF16),
            pltpu.VMEM((HEAD_SIZE, WINDOW), BF16),
            pltpu.VMEM((D, ROWS), BF16),
            pltpu.VMEM((D // 2, ROWS), BF16),
            pltpu.VMEM((FEATURES, ROWS), BF16),
            pltpu.VMEM((2 * FEATURES, ROWS), BF16),
            pltpu.VMEM((64, ROWS), F32),
            pltpu.SMEM((3,), F32),
            pltpu.VMEM((FEATURES,), BF16),
            dma((9,)), dma((11,)), dma((11,)), dma((2,)), dma((2,)), dma((80,)), dma((80,)),
            dma((16,)), dma((16,)), dma((20,)), dma((20,)), dma((7,)), dma((7,)),
            dma((32,)), dma((32,)), dma((8,)), dma((8,)), dma((16,)), dma((16,)),
        ],
        compiler_params=pltpu.CompilerParams(
            collective_id=0, has_side_effects=True, vmem_limit_bytes=60 * 2**20
        ),
    )(
        queries.T, key_heads.T, projected_value_heads.T, sink_logit_table, out_weight,
        residual, norm_gain, up_weight, down_weight.T,
    )


def solution(mesh):
    return jax.shard_map(
        body,
        mesh=mesh,
        in_specs=(
            P("sp", "tp"), P("sp", "tp"), P("sp", "tp"), P("tp"), P("tp", None),
            P("sp", "tp"), P("tp"), P("sp", "tp"), P("tp", "sp"),
        ),
        out_specs=P("sp", "tp"),
        check_vma=False,
    )
```

```python
import functools

import jax
import jax.numpy as jnp
from jax import lax
from jax.experimental import pallas as pl
from jax.experimental.pallas import tpu as pltpu
from jax.sharding import PartitionSpec as P

D = 3072
HEAD_SIZE = 64
WINDOW = 128
EPSILON = 1e-06

ROWS = 1024
FEATURES = 384
HEADS = 192
SHARD = 192
HALF = 96
QUARTER = 48
HIDDEN = 1536
TILE = 256

MESH = pl.DeviceIdType.MESH
BF16 = jnp.bfloat16
F32 = jnp.float32


def dot(a, b, dims):
    return lax.dot_general(a, b, (dims, ((), ())), preferred_element_type=F32)


def kernel(
    queries, keys, values, sinks_in, out_weight, residual, gains_in, up, down,
    result,
    up_all, down_all, x_all, att_all, w_all, w_pass, hidden, act_t, mixed, stream, res_v,
    q_v, k_v, v_v, halo_k, halo_v, partials, paired, chained, final, squares, sink, gain,
    local_sem, w_send, w_recv, halo_send, halo_recv, g_send, g_recv,
    att_send, att_recv, x_send, x_recv, sq_send, sq_recv,
    pair_send, pair_recv, side_send, side_recv, owner_send, owner_recv,
):
    s, t = lax.axis_index("sp"), lax.axis_index("tp")
    z, x = s // 4, s % 4
    y, c = t // 2, t % 2

    def ring(position, by):
        return (position + by + 4) % 4

    def device(zz, xx, yy, cc):
        return (zz * 4 + xx, yy * 2 + cc)

    partner = (s, y * 2 + (1 - c))
    y_next = {1: (s, ring(y, 1) * 2 + c), -1: (s, ring(y, -1) * 2 + c)}
    DIRS = ((0, 1), (1, -1))

    def remote(src, dst, send, recv, target):
        return pltpu.make_async_remote_copy(
            src_ref=src, dst_ref=dst, send_sem=send, recv_sem=recv,
            device_id=target, device_id_type=MESH,
        )

    def start(copy):
        copy.start()

    def arrived(ref, sem):
        remote(ref, ref, sem, sem, partner).wait_recv()

    def sent(ref, sem):
        remote(ref, ref, sem, sem, partner).wait_send()

    barrier = pltpu.get_barrier_semaphore()
    greeted = [
        device(z, ring(x, 1), y, c), device(z, ring(x, -1), y, c),
        device(ring(z, 1), x, y, c), device(ring(z, -1), x, y, c),
        ((s + 1) % 16, t), ((s + 15) % 16, t),
    ] + [(s, (t + k) % 8) for k in range(1, 8)]
    for other in greeted:
        pl.semaphore_signal(barrier, inc=1, device_id=other, device_id_type=MESH)
    locals_ = [
        pltpu.make_async_copy(src, dst, local_sem.at[i])
        for i, (src, dst) in enumerate([
            (queries, q_v), (keys, k_v), (values, v_v), (sinks_in, sink), (gains_in, gain), (residual, res_v),
            (up, up_all.at[pl.ds(pl.multiple_of(s * SHARD, SHARD), SHARD)]),
            (down, down_all.at[pl.ds(pl.multiple_of(s * SHARD, SHARD), SHARD)]),
            (out_weight.at[:, pl.ds(pl.multiple_of(t * FEATURES, 128), FEATURES)],
             w_all.at[pl.ds(pl.multiple_of(t * HEADS, HEADS), HEADS)]),
        ])
    ]
    for copy in locals_:
        copy.start()
    pl.semaphore_wait(barrier, len(greeted))

    STEPS = (0, -1, 1, 2)
    ORDER = ((0, 1, 2, 3), (0, 1, 3, 2))

    class Gather:
        def __init__(self, own, buf, base):
            self.own, self.buf, self.base = own, buf, base

        def spot(self, half, sec, prim, low, count):
            zz, xx = (sec, prim) if half == 0 else (prim, sec)
            row = (zz * 4 + xx) * SHARD + half * HALF + low
            return self.buf.at[pl.ds(pl.multiple_of(row, 16), count)]

        def copy(self, half, index, src, dst, target):
            if index < 4:
                step = index // 2
            else:
                step = 2 + 4 * (index >= 12) + ORDER[half].index((index - 4) // 2 % 4)
            return remote(src, dst, g_send.at[self.base], g_recv.at[self.base * 10 + step], target)

        def arrived(self, step, rows):
            arrived(self.buf.at[pl.ds(0, rows)], g_recv.at[self.base * 10 + step])

        def at(self, half):
            return (z, x) if half == 0 else (x, z)

        def towards(self, half, primary, by):
            if primary == (half == 0):
                return device(z, ring(x, by), y, c)
            return device(ring(z, by), x, y, c)

        def first(self):
            for half in (0, 1):
                sec, prim = self.at(half)
                src = self.own.at[pl.ds(half * HALF, HALF)]
                dst = self.spot(half, sec, prim, 0, HALF)
                for d, by in DIRS:
                    start(self.copy(half, d, src, dst, self.towards(half, True, by)))
            for half in (0, 1):
                sec, prim = self.at(half)
                src = self.own.at[pl.ds(half * HALF, HALF)]
                dst = self.spot(half, sec, prim, 0, HALF)
                for d, by in DIRS:
                    start(self.copy(half, 4 + d, src, dst, self.towards(half, False, by)))

        def second(self):
            self.arrived(0, 4 * HALF)
            for half in (0, 1):
                sec, prim = self.at(half)
                for d, by in DIRS:
                    origin = ring(prim, -by)
                    piece = self.spot(half, sec, origin, d * QUARTER, QUARTER)
                    start(self.copy(half, 2 + d, piece, piece, self.towards(half, True, by)))
            for half in (0, 1):
                self.spread(half, 1)

        def spread(self, half, j):
            sec, prim = self.at(half)
            piece = self.spot(half, sec, ring(prim, STEPS[j]), 0, HALF)
            for d, by in DIRS:
                start(self.copy(half, 4 + 2 * j + d, piece, piece, self.towards(half, False, by)))

        def third(self):
            self.spread(0, 2)
            self.arrived(1, 4 * QUARTER)
            self.spread(1, 3)

        def fourth(self):
            self.spread(1, 2)
            self.spread(0, 3)

        def forward(self, k):
            self.arrived(2 + k, 4 * HALF)
            for half in (0, 1):
                j = ORDER[half][k]
                sec, prim = self.at(half)
                origin = ring(prim, STEPS[j])
                for d, by in DIRS:
                    piece = self.spot(half, ring(sec, -by), origin, d * QUARTER, QUARTER)
                    start(self.copy(half, 12 + 2 * j + d, piece, piece, self.towards(half, False, by)))

        def last(self, k):
            self.arrived(6 + k, 4 * QUARTER)

        def sent(self):
            sent(self.buf.at[pl.ds(0, 15 * SHARD)], g_send.at[self.base])

    up_gather = Gather(up, up_all, 0)
    down_gather = Gather(down, down_all, 1)
    after = ((s + 1) % 16, t)
    tail = pl.ds(ROWS - WINDOW, WINDOW)
    halo_copies = [
        remote(keys.at[:, tail], halo_k, halo_send.at[0], halo_recv.at[0], after),
        remote(values.at[:, tail], halo_v, halo_send.at[1], halo_recv.at[1], after),
    ]
    for copy in halo_copies:
        start(copy)
    up_gather.first()

    def w_cols(yy, cc=0, count=FEATURES):
        return pl.ds(pl.multiple_of((yy * 2 + cc) * FEATURES, 128), count)

    def w_rows(yy, cc, low=0, count=HEADS):
        return w_all.at[pl.ds(pl.multiple_of((yy * 2 + cc) * HEADS + low, 32), count)]

    def w_relay(k, by):
        src = out_weight.at[pl.ds(k * HALF, HALF), w_cols(ring(y, 2), 0, 2 * FEATURES)]
        return remote(src, w_pass.at[k], w_send.at[0], w_recv.at[0], y_next[by])

    for k, by in DIRS:
        start(w_relay(k, by))
    start(remote(out_weight.at[:, w_cols(y, 1 - c)], w_rows(y, c), w_send.at[1], w_recv.at[1], partner))
    for k, by in DIRS:
        for cc in (0, 1):
            start(remote(
                out_weight.at[:, w_cols(ring(y, by), cc)], w_rows(y, c),
                w_send.at[1], w_recv.at[2 + k], (s, ring(y, by) * 2 + cc),
            ))

    def w_pass_on():
        arrived(w_pass, w_recv.at[0])
        for k, by in DIRS:
            for cc in (0, 1):
                start(remote(
                    w_pass.at[k, :, pl.ds(cc * FEATURES, FEATURES)], w_rows(ring(y, -by), c, k * HALF, HALF),
                    w_send.at[1], w_recv.at[4], (s, ring(y, by) * 2 + cc),
                ))

    key_at = lax.broadcasted_iota(jnp.int32, (2 * WINDOW, 3 * WINDOW), 0)
    query_at = lax.broadcasted_iota(jnp.int32, (2 * WINDOW, 3 * WINDOW), 1) % WINDOW
    mine_row = t * HEADS

    def attend(n, key_band, value_band, allowed):
        lanes = pl.ds(pl.multiple_of(n * WINDOW, WINDOW), WINDOW)
        q = jnp.concatenate([q_v[pl.ds(g * HEAD_SIZE, HEAD_SIZE), lanes] for g in range(3)], axis=1)
        scores = dot(key_band, q, ((0,), (0,))) * HEAD_SIZE**-0.5
        masked = jnp.where(allowed, scores, -1e30)
        top = jnp.maximum(jnp.max(masked, axis=0, keepdims=True), sinks)
        powers = jnp.where(allowed, jnp.exp(masked - top), 0.0)
        denom = jnp.sum(powers, axis=0, keepdims=True) + jnp.exp(sinks - top)
        probs = (powers * (1.0 / denom)).astype(BF16)
        output = dot(value_band, probs, ((1,), (0,))).astype(BF16)
        for g in range(3):
            rows = pl.ds(pl.multiple_of(mine_row + g * HEAD_SIZE, HEAD_SIZE), HEAD_SIZE)
            att_all[rows, lanes] = output[:, g * WINDOW : (g + 1) * WINDOW]

    near = (key_at > query_at) & (key_at <= query_at + WINDOW)
    for copy in locals_[:4]:
        copy.wait()
    sinks = jnp.concatenate([jnp.full((1, WINDOW), sink[g], F32) for g in range(3)], axis=1)

    def attend_blocks(low, high):
        @pl.loop(low, high)
        def _(n):
            band = pl.ds(pl.multiple_of((n - 1) * WINDOW, WINDOW), 2 * WINDOW)
            attend(n, k_v[:, band], v_v[:, band], near)

    PART = ROWS // 2
    FIRST = (PART, 0)

    def att_rows(yy, cc, part, low=0, count=HEADS):
        row = (yy * 2 + cc) * HEADS + low
        return att_all.at[pl.ds(pl.multiple_of(row, 32), count), pl.ds(FIRST[part], PART)]

    def att_copy(part, index, ref, target):
        k = part * 7 + (0, 1, 2, 2, 3, 4, 5, 6)[index]
        return remote(ref, ref, att_send.at[0], att_recv.at[k], target)

    def att_arrived(part, index, ref):
        att_copy(part, index, ref, partner).wait_recv()

    def att_begin(part):
        for d, by in DIRS:
            start(att_copy(part, d, att_rows(y, c, part), y_next[by]))

    def att_pass(part):
        for d, by in DIRS:
            near_y = ring(y, -by)
            att_arrived(part, d, att_rows(near_y, c, part))
            start(att_copy(part, 2 + d, att_rows(near_y, c, part, d * HALF, HALF), y_next[by]))
            start(att_copy(part, 5 + d, att_rows(near_y, c, part), partner))

    def mix(yy, part, first):
        rows = pl.ds(pl.multiple_of(yy * 2 * HEADS, 2 * HEADS), 2 * HEADS)

        @pl.loop(0, PART // TILE)
        def _(i):
            tokens = pl.ds(pl.multiple_of(FIRST[part] + i * TILE, TILE), TILE)
            total = dot(att_all[rows, tokens], w_all[rows, :], ((0,), (0,)))
            mixed[tokens, :] = total if first else mixed[tokens, :] + total

    def mix_near(part):
        for d, by in DIRS:
            near_y = ring(y, -by)
            att_arrived(part, 5 + d, att_rows(near_y, 1 - c, part))
            if part == 0:
                arrived(w_rows(near_y, 0, 0, 2 * HEADS), w_recv.at[2 + d])
            mix(near_y, part, False)

    def mix_far(part):
        far = ring(y, 2)
        att_arrived(part, 2, att_rows(far, c, part))
        start(att_copy(part, 7, att_rows(far, c, part), partner))
        if part == 0:
            arrived(w_rows(far, 0, 0, 2 * HEADS), w_recv.at[4])
        att_arrived(part, 7, att_rows(far, 1 - c, part))
        mix(far, part, False)

    lanes_of = lambda cc: pl.ds(pl.multiple_of(cc * FEATURES, 128), FEATURES)

    def x_block(yy, cc, part, quarter=None):
        low, count = (0, PART) if quarter is None else (quarter * TILE, TILE)
        return x_all.at[pl.ds(pl.multiple_of(yy * ROWS + FIRST[part] + low, TILE), count), lanes_of(cc)]

    ones = jnp.ones((8, FEATURES), BF16)
    sq_rows = pl.ds(pl.multiple_of(t * 8, 8), 8)

    def make_x(part):
        gains = gain[...].astype(F32).reshape(1, FEATURES)

        @pl.loop(0, PART // TILE)
        def _(i):
            tokens = pl.ds(pl.multiple_of(FIRST[part] + i * TILE, TILE), TILE)
            here = (res_v[tokens, :].astype(F32) + mixed[tokens, :]).astype(BF16)
            stream[tokens, :] = here
            wide = here.astype(F32)
            rows = pl.ds(pl.multiple_of(y * ROWS + FIRST[part] + i * TILE, TILE), TILE)
            x_all[rows, lanes_of(c)] = (wide * gains).astype(BF16)
            sq = wide * wide
            high = sq.astype(BF16)
            low = (sq - high.astype(F32)).astype(BF16)
            squares[sq_rows, tokens] = dot(ones, high, ((1,), (1,))) + dot(ones, low, ((1,), (1,)))

    def x_copy(part, index, ref, target):
        k = part * 7 + (0, 0, 1, 1, 2, 2, 3, 4, 5, 6)[index]
        return remote(ref, ref, x_send.at[0], x_recv.at[k], target)

    def x_arrived(part, index, ref):
        x_copy(part, index, ref, partner).wait_recv()

    def x_begin(part, second):
        for d, by in DIRS:
            quarter = 1 - d if second else d
            start(x_copy(part, 2 * second + d, x_block(y, c, part, quarter), y_next[by]))

    def x_pass(part):
        x_arrived(part, 0, x_block(y, c, part))
        for d, by in DIRS:
            start(x_copy(part, 4 + d, x_block(ring(y, -by), c, part, d), y_next[by]))

    def x_near(part):
        x_arrived(part, 2, x_block(y, c, part))
        for d, by in DIRS:
            start(x_copy(part, 7 + d, x_block(ring(y, -by), c, part), partner))

    def x_far(part):
        x_arrived(part, 4, x_block(ring(y, 2), c, part))
        start(x_copy(part, 9, x_block(ring(y, 2), c, part), partner))

    def hide(yy, part, first=False, last=False):
        @pl.loop(0, PART // TILE)
        def _(i):
            tokens = pl.ds(pl.multiple_of(FIRST[part] + i * TILE, TILE), TILE)
            rows = pl.ds(pl.multiple_of(yy * ROWS + FIRST[part] + i * TILE, TILE), TILE)
            for n in range(3):
                cols = pl.ds(n * 512, 512)
                total = dot(x_all[rows, :], up_all[pl.ds(pl.multiple_of(yy * 768, 768), 768), cols], ((1,), (0,)))
                if not first:
                    total = total + hidden[tokens, cols]
                if last:
                    units = jnp.square(jnp.maximum(total, 0.0)).astype(BF16)
                    act_t[cols, tokens] = jnp.transpose(units)
                else:
                    hidden[tokens, cols] = total

    attend_blocks(4, 8)
    att_begin(0)
    start(att_copy(0, 4, att_rows(y, c, 0), partner))
    attend_blocks(1, 4)
    for copy in halo_copies:
        copy.wait_recv()
    first_key = jnp.where(s == 0, WINDOW, 0)
    attend(
        0,
        jnp.concatenate([halo_k[...], k_v[:, 0:WINDOW]], axis=1),
        jnp.concatenate([halo_v[...], v_v[:, 0:WINDOW]], axis=1),
        near & (key_at >= first_key),
    )
    start(att_copy(1, 4, att_rows(y, c, 1), partner))
    w_pass_on()
    up_gather.second()
    for copy in locals_[4:]:
        copy.wait()
    arrived(w_rows(y, 1 - c), w_recv.at[1])
    for part in (0, 1):
        att_arrived(part, 4, att_rows(y, 1 - c, part))
        mix(y, part, True)
    att_pass(0)
    att_begin(1)
    up_gather.forward(0)
    up_gather.third()
    mix_near(0)
    mix_far(0)
    make_x(0)
    x_begin(0, False)
    att_pass(1)
    x_begin(0, True)
    start(x_copy(0, 6, x_block(y, c, 0), partner))
    up_gather.forward(1)
    up_gather.fourth()
    mix_near(1)
    x_pass(0)
    mix_far(1)
    make_x(1)
    x_begin(1, False)
    x_begin(1, True)
    start(x_copy(1, 6, x_block(y, c, 1), partner))
    for k in range(1, 8):
        ref = squares.at[sq_rows]
        start(remote(ref, ref, sq_send.at[0], sq_recv.at[0], (s, (t + k) % 8)))
    x_near(0)
    up_gather.forward(2)
    x_far(0)
    up_gather.last(0)
    x_arrived(0, 6, x_block(y, 1 - c, 0))
    for d, by in DIRS:
        x_arrived(0, 7 + d, x_block(ring(y, -by), 1 - c, 0))
    x_arrived(0, 9, x_block(ring(y, 2), 1 - c, 0))
    hide(z, 0, first=True)
    up_gather.forward(3)
    down_gather.first()
    x_pass(1)
    up_gather.last(1)
    hide(ring(z, -1), 0)
    x_near(1)
    up_gather.last(2)
    up_gather.last(3)
    hide(ring(z, 1), 0)
    hide(ring(z, 2), 0, last=True)
    x_far(1)
    x_arrived(1, 6, x_block(y, 1 - c, 1))
    hide(y, 1, first=True)
    for d, by in DIRS:
        x_arrived(1, 7 + d, x_block(ring(y, -by), 1 - c, 1))
        hide(ring(y, -by), 1)
        if d == 0:
            down_gather.second()
    x_arrived(1, 9, x_block(ring(y, 2), 1 - c, 1))
    hide(ring(y, 2), 1, last=True)

    GROUPS = [[(half, 0, j) for j in range(3)] for half in (0, 1)]
    GROUPS.append([(half, 0, 3) for half in (0, 1)])
    for k in range(4):
        GROUPS.append([(half, i, ORDER[half][k]) for half in (0, 1) for i in (1, 2)])
        GROUPS.append([(half, 3, ORDER[half][k]) for half in (0, 1)])

    def lanes(part):
        return pl.ds(pl.multiple_of(part * PART, PART), PART)

    class Piece:
        def __init__(self, half, i, j):
            sec, prim = down_gather.at(half)
            sec, prim = ring(sec, STEPS[i]), ring(prim, STEPS[j])
            zz, xx = (sec, prim) if half == 0 else (prim, sec)
            self.row = (zz * 4 + xx) * SHARD + half * HALF
            self.half = half
            self.part = (xx % 2) * 2 + half
            self.mine = xx // 2 == c
            self.away = (y - zz + 4) % 4
            self.pair = zz * 4 + self.part

        def rows(self, low=0, count=HALF):
            return pl.ds(pl.multiple_of(self.row + low, 16), count)

        def paired_rows(self, low=0, count=HALF):
            return pl.ds(pl.multiple_of(self.pair * HALF + low, 16), count)

        def to_pair(self, part):
            k = self.pair * 2 + part
            return remote(
                partials.at[self.rows(), lanes(part)], paired.at[self.paired_rows(), lanes(part)],
                pair_send.at[0], pair_recv.at[k], partner,
            )

        def to_side(self, part):
            k = self.part * 2 + part
            return remote(
                partials.at[self.rows(), lanes(part)],
                chained.at[pl.ds(pl.multiple_of(self.part * HALF, 32), HALF), lanes(part)],
                side_send.at[0], side_recv.at[k], y_next[-1 if self.half == 0 else 1],
            )

        def to_owner(self, part):
            index = (self.away // 2) * 4 + self.part
            return remote(
                partials.at[self.rows(), lanes(part)],
                final.at[pl.ds(pl.multiple_of(index * HALF, 32), HALF), lanes(part)],
                owner_send.at[0], owner_recv.at[part], (s, ring(y, -self.away) * 2 + c),
            )

        def add(self, part, side):
            rows = self.rows()
            total = partials[rows, lanes(part)].astype(F32) + paired[self.paired_rows(), lanes(part)].astype(F32)
            if side:
                there = pl.ds(pl.multiple_of(self.part * HALF, 32), HALF)
                total = total + chained[there, lanes(part)].astype(F32)
            partials[rows, lanes(part)] = total.astype(BF16)

    groups = [[Piece(*facts) for facts in group] for group in GROUPS]

    def compute(group):
        @pl.loop(0, 2)
        def _(part):
            @pl.loop(0, PART // TILE)
            def _(i):
                tokens = pl.ds(pl.multiple_of(part * PART + i * TILE, TILE), TILE)
                weight = jnp.concatenate([down_all[p.rows(), :] for p in group], axis=0)
                total = dot(weight, act_t[:, tokens], ((1,), (0,))).astype(BF16)
                for k, p in enumerate(group):
                    partials[p.rows(), tokens] = total[k * HALF : (k + 1) * HALF]

            for p in group:
                @pl.when(jnp.logical_not(p.mine))
                def _():
                    p.to_pair(part).start()

    def combine(group):
        @pl.loop(0, 2)
        def _(part):
            for p in group:
                side = 1 if p.half == 0 else 3

                @pl.when(p.mine & (p.away != 0) & (p.away != side))
                def _():
                    p.to_pair(part).wait_recv()
                    p.add(part, False)

                    @pl.when(p.away == 2)
                    def _():
                        p.to_side(part).start()

                    @pl.when(p.away != 2)
                    def _():
                        p.to_owner(part).start()

    def relay(group):
        @pl.loop(0, 2)
        def _(part):
            for p in group:
                @pl.when(p.mine & (p.away == (1 if p.half == 0 else 3)))
                def _():
                    p.to_pair(part).wait_recv()
                    p.to_side(part).wait_recv()
                    p.add(part, True)
                    p.to_owner(part).start()

    compute(groups[0])
    compute(groups[1])
    combine(groups[0])
    down_gather.forward(0)
    compute(groups[3])
    combine(groups[1])
    down_gather.third()
    compute(groups[2])
    combine(groups[3])
    combine(groups[2])
    down_gather.forward(1)
    down_gather.fourth()
    compute(groups[5])
    relay(groups[0])
    relay(groups[1])
    down_gather.last(0)
    combine(groups[5])
    compute(groups[4])
    combine(groups[4])
    relay(groups[3])
    for copy in halo_copies:
        copy.wait_send()
    sent(w_pass, w_send.at[0])
    sent(w_all.at[pl.ds(0, 7 * HEADS)], w_send.at[1])
    sent(att_all.at[pl.ds(0, 7 * HEADS)], att_send.at[0])
    sent(x_all.at[pl.ds(0, 7 * PART)], x_send.at[0])
    sent(squares.at[pl.ds(0, 56)], sq_send.at[0])
    up_gather.sent()
    down_gather.forward(2)
    compute(groups[7])
    relay(groups[2])
    combine(groups[7])
    down_gather.last(1)
    compute(groups[6])
    combine(groups[6])
    relay(groups[5])
    relay(groups[4])
    down_gather.forward(3)
    compute(groups[9])
    combine(groups[9])
    relay(groups[7])
    down_gather.last(2)
    compute(groups[8])
    combine(groups[8])
    relay(groups[6])
    down_gather.last(3)
    compute(groups[10])
    combine(groups[10])
    relay(groups[9])
    relay(groups[8])
    relay(groups[10])
    down_gather.sent()
    sent(paired, pair_send.at[0])

    arrived(squares.at[pl.ds(0, 56)], sq_recv.at[0])
    own = [Piece(half, 0, 0) for half in (0, 1, 0, 1)]
    for part, p in enumerate(own):
        p.part = part
        p.half = part % 2
        p.row = (y * 4 + c * 2) * SHARD + part * HALF
        p.pair = y * 4 + part
    mine = pl.ds(pl.multiple_of((y * 4 + c * 2) * SHARD, FEATURES), FEATURES)
    beside = pl.ds(pl.multiple_of(y * FEATURES, FEATURES), FEATURES)

    @pl.loop(0, 2)
    def _(part):
        for p in own:
            p.to_pair(part).wait_recv()
        arrived(final.at[pl.ds(0, FEATURES)], owner_recv.at[part])

        @pl.loop(0, PART // 128)
        def _(i):
            tokens = pl.ds(pl.multiple_of(part * PART + i * 128, 128), 128)
            total = partials[mine, tokens].astype(F32) + paired[beside, tokens].astype(F32)
            for k in range(2):
                total = total + final[k * FEATURES : (k + 1) * FEATURES, tokens].astype(F32)
            norm = squares[0:1, tokens]
            for k in range(1, 8):
                norm = norm + squares[8 * k : 8 * k + 1, tokens]
            total = total * (1.0 / (norm * (1.0 / D) + EPSILON))
            result[tokens, :] = (stream[tokens, :].astype(F32) + jnp.transpose(total)).astype(BF16)

    sent(chained, side_send.at[0])
    sent(final, owner_send.at[0])


def body(
    queries, key_heads, projected_value_heads, sink_logit_table, out_weight,
    residual, norm_gain, up_weight, down_weight,
):
    hbm = pl.BlockSpec(memory_space=pl.ANY)
    dma = pltpu.SemaphoreType.DMA
    return pl.pallas_call(
        kernel,
        out_shape=pltpu.VMEM((ROWS, FEATURES), BF16),
        in_specs=[hbm] * 9,
        out_specs=pl.BlockSpec(memory_space=pltpu.VMEM),
        scratch_shapes=[
            pltpu.VMEM((D, HIDDEN), BF16),
            pltpu.VMEM((D, HIDDEN), BF16),
            pltpu.VMEM((4 * ROWS, 2 * FEATURES), BF16),
            pltpu.VMEM((8 * HEADS, ROWS), BF16),
            pltpu.VMEM((8 * HEADS, FEATURES), BF16),
            pltpu.VMEM((2, HALF, 2 * FEATURES), BF16),
            pltpu.VMEM((ROWS, HIDDEN), F32),
            pltpu.VMEM((HIDDEN, ROWS), BF16),
            pltpu.VMEM((ROWS, FEATURES), F32),
            pltpu.VMEM((ROWS, FEATURES), BF16),
            pltpu.VMEM((ROWS, FEATURES), BF16),
            pltpu.VMEM((HEADS, ROWS), BF16),
            pltpu.VMEM((HEAD_SIZE, ROWS), BF16),
            pltpu.VMEM((HEAD_SIZE, ROWS), BF16),
            pltpu.VMEM((HEAD_SIZE, WINDOW), BF16),
            pltpu.VMEM((HEAD_SIZE, WINDOW), BF16),
            pltpu.VMEM((D, ROWS), BF16),
            pltpu.VMEM((D // 2, ROWS), BF16),
            pltpu.VMEM((FEATURES, ROWS), BF16),
            pltpu.VMEM((2 * FEATURES, ROWS), BF16),
            pltpu.VMEM((64, ROWS), F32),
            pltpu.SMEM((3,), F32),
            pltpu.VMEM((FEATURES,), BF16),
            dma((9,)), dma((2,)), dma((5,)), dma((2,)), dma((2,)), dma((2,)), dma((20,)),
            dma((1,)), dma((14,)), dma((1,)), dma((14,)), dma((1,)), dma((1,)),
            dma((1,)), dma((32,)), dma((1,)), dma((8,)), dma((1,)), dma((2,)),
        ],
        compiler_params=pltpu.CompilerParams(
            collective_id=0, has_side_effects=True, vmem_limit_bytes=60 * 2**20
        ),
    )(
        queries.T, key_heads.T, projected_value_heads.T, sink_logit_table, out_weight,
        residual, norm_gain, up_weight, down_weight.T,
    )


def solution(mesh):
    return jax.shard_map(
        body,
        mesh=mesh,
        in_specs=(
            P("sp", "tp"), P("sp", "tp"), P("sp", "tp"), P("tp"), P("tp", None),
            P("sp", "tp"), P("tp"), P("sp", "tp"), P("tp", "sp"),
        ),
        out_specs=P("sp", "tp"),
        check_vma=False,
    )
```

```python
import functools

import jax
import jax.numpy as jnp
from jax import lax
from jax.experimental import pallas as pl
from jax.experimental.pallas import tpu as pltpu
from jax.sharding import PartitionSpec as P

D = 3072
HEAD_SIZE = 64
WINDOW = 128
EPSILON = 1e-06

ROWS = 1024
FEATURES = 384
HEADS = 192
SHARD = 192
HALF = 96
QUARTER = 48
HIDDEN = 1536
TILE = 256

MESH = pl.DeviceIdType.MESH
BF16 = jnp.bfloat16
F32 = jnp.float32


def dot(a, b, dims):
    return lax.dot_general(a, b, (dims, ((), ())), preferred_element_type=F32)


def kernel(
    queries, keys, values, sinks_in, out_weight, residual, gains_in, up, down,
    result,
    up_all, down_all, x_all, att_all, w_all, w_pass, hidden, act_t, mixed, stream, res_v,
    q_v, k_v, v_v, halo_k, halo_v, partials, paired, chained, final, squares, sink, gain,
    local_sem, w_send, w_recv, halo_send, halo_recv, g_send, g_recv,
    att_send, att_recv, x_send, x_recv, sq_send, sq_recv,
    pair_send, pair_recv, side_send, side_recv, owner_send, owner_recv,
):
    s, t = lax.axis_index("sp"), lax.axis_index("tp")
    z, x = s // 4, s % 4
    y, c = t // 2, t % 2

    def ring(position, by):
        return (position + by + 4) % 4

    def device(zz, xx, yy, cc):
        return (zz * 4 + xx, yy * 2 + cc)

    partner = (s, y * 2 + (1 - c))
    y_next = {1: (s, ring(y, 1) * 2 + c), -1: (s, ring(y, -1) * 2 + c)}
    DIRS = ((0, 1), (1, -1))

    def remote(src, dst, send, recv, target):
        return pltpu.make_async_remote_copy(
            src_ref=src, dst_ref=dst, send_sem=send, recv_sem=recv,
            device_id=target, device_id_type=MESH,
        )

    def start(copy):
        copy.start()

    def arrived(ref, sem):
        remote(ref, ref, sem, sem, partner).wait_recv()

    def sent(ref, sem):
        remote(ref, ref, sem, sem, partner).wait_send()

    barrier = pltpu.get_barrier_semaphore()
    greeted = [
        device(z, ring(x, 1), y, c), device(z, ring(x, -1), y, c),
        device(ring(z, 1), x, y, c), device(ring(z, -1), x, y, c),
        ((s + 1) % 16, t), ((s + 15) % 16, t),
    ] + [(s, (t + k) % 8) for k in range(1, 8)]
    for other in greeted:
        pl.semaphore_signal(barrier, inc=1, device_id=other, device_id_type=MESH)
    locals_ = [
        pltpu.make_async_copy(src, dst, local_sem.at[i])
        for i, (src, dst) in enumerate([
            (up, up_all.at[pl.ds(pl.multiple_of(s * SHARD, SHARD), SHARD)]),
            (queries, q_v), (keys, k_v), (values, v_v), (sinks_in, sink), (gains_in, gain), (residual, res_v),
            (down, down_all.at[pl.ds(pl.multiple_of(s * SHARD, SHARD), SHARD)]),
            (out_weight.at[:, pl.ds(pl.multiple_of(t * FEATURES, 128), FEATURES)],
             w_all.at[pl.ds(pl.multiple_of(t * HEADS, HEADS), HEADS)]),
        ])
    ]
    for copy in locals_:
        copy.start()
    pl.semaphore_wait(barrier, len(greeted))

    STEPS = (0, -1, 1, 2)
    ORDER = ((0, 1, 2, 3), (0, 1, 3, 2))

    class Gather:
        def __init__(self, own, buf, base):
            self.own, self.buf, self.base = own, buf, base

        def spot(self, half, sec, prim, low, count):
            zz, xx = (sec, prim) if half == 0 else (prim, sec)
            row = (zz * 4 + xx) * SHARD + half * HALF + low
            return self.buf.at[pl.ds(pl.multiple_of(row, 16), count)]

        def copy(self, half, index, src, dst, target):
            if index < 4:
                step = index // 2
            else:
                step = 2 + 4 * (index >= 12) + ORDER[half].index((index - 4) // 2 % 4)
            return remote(src, dst, g_send.at[self.base], g_recv.at[self.base * 10 + step], target)

        def arrived(self, step, rows):
            arrived(self.buf.at[pl.ds(0, rows)], g_recv.at[self.base * 10 + step])

        def at(self, half):
            return (z, x) if half == 0 else (x, z)

        def towards(self, half, primary, by):
            if primary == (half == 0):
                return device(z, ring(x, by), y, c)
            return device(ring(z, by), x, y, c)

        def first(self):
            for half in (0, 1):
                sec, prim = self.at(half)
                src = self.own.at[pl.ds(half * HALF, HALF)]
                dst = self.spot(half, sec, prim, 0, HALF)
                for d, by in DIRS:
                    start(self.copy(half, d, src, dst, self.towards(half, True, by)))
            for half in (0, 1):
                sec, prim = self.at(half)
                src = self.own.at[pl.ds(half * HALF, HALF)]
                dst = self.spot(half, sec, prim, 0, HALF)
                for d, by in DIRS:
                    start(self.copy(half, 4 + d, src, dst, self.towards(half, False, by)))

        def second(self):
            self.arrived(0, 4 * HALF)
            for half in (0, 1):
                sec, prim = self.at(half)
                for d, by in DIRS:
                    origin = ring(prim, -by)
                    piece = self.spot(half, sec, origin, d * QUARTER, QUARTER)
                    start(self.copy(half, 2 + d, piece, piece, self.towards(half, True, by)))
            for half in (0, 1):
                self.spread(half, 1)

        def spread(self, half, j):
            sec, prim = self.at(half)
            piece = self.spot(half, sec, ring(prim, STEPS[j]), 0, HALF)
            for d, by in DIRS:
                start(self.copy(half, 4 + 2 * j + d, piece, piece, self.towards(half, False, by)))

        def third(self):
            self.spread(0, 2)
            self.arrived(1, 4 * QUARTER)
            self.spread(1, 3)

        def fourth(self):
            self.spread(1, 2)
            self.spread(0, 3)

        def forward(self, k):
            self.arrived(2 + k, 4 * HALF)
            for half in (0, 1):
                j = ORDER[half][k]
                sec, prim = self.at(half)
                origin = ring(prim, STEPS[j])
                for d, by in DIRS:
                    piece = self.spot(half, ring(sec, -by), origin, d * QUARTER, QUARTER)
                    start(self.copy(half, 12 + 2 * j + d, piece, piece, self.towards(half, False, by)))

        def last(self, k):
            self.arrived(6 + k, 4 * QUARTER)

        def sent(self):
            sent(self.buf.at[pl.ds(0, 15 * SHARD)], g_send.at[self.base])

    up_gather = Gather(up_all.at[pl.ds(pl.multiple_of(s * SHARD, SHARD), SHARD)], up_all, 0)
    down_gather = Gather(down, down_all, 1)
    after = ((s + 1) % 16, t)
    tail = pl.ds(ROWS - WINDOW, WINDOW)
    halo_copies = [
        remote(keys.at[:, tail], halo_k, halo_send.at[0], halo_recv.at[0], after),
        remote(values.at[:, tail], halo_v, halo_send.at[1], halo_recv.at[1], after),
    ]
    for copy in halo_copies:
        start(copy)
    locals_[0].wait()
    up_gather.first()

    def w_cols(yy, cc=0, count=FEATURES):
        return pl.ds(pl.multiple_of((yy * 2 + cc) * FEATURES, 128), count)

    def w_rows(yy, cc, low=0, count=HEADS):
        return w_all.at[pl.ds(pl.multiple_of((yy * 2 + cc) * HEADS + low, 32), count)]

    def w_relay(k, by):
        src = out_weight.at[pl.ds(k * HALF, HALF), w_cols(ring(y, 2), 0, 2 * FEATURES)]
        return remote(src, w_pass.at[k], w_send.at[0], w_recv.at[0], y_next[by])

    for k, by in DIRS:
        start(w_relay(k, by))
    start(remote(out_weight.at[:, w_cols(y, 1 - c)], w_rows(y, c), w_send.at[1], w_recv.at[1], partner))
    for k, by in DIRS:
        for cc in (0, 1):
            start(remote(
                out_weight.at[:, w_cols(ring(y, by), cc)], w_rows(y, c),
                w_send.at[1], w_recv.at[2 + k], (s, ring(y, by) * 2 + cc),
            ))

    def w_pass_on():
        arrived(w_pass, w_recv.at[0])
        for k, by in DIRS:
            for cc in (0, 1):
                start(remote(
                    w_pass.at[k, :, pl.ds(cc * FEATURES, FEATURES)], w_rows(ring(y, -by), c, k * HALF, HALF),
                    w_send.at[1], w_recv.at[4], (s, ring(y, by) * 2 + cc),
                ))

    key_at = lax.broadcasted_iota(jnp.int32, (2 * WINDOW, 3 * WINDOW), 0)
    query_at = lax.broadcasted_iota(jnp.int32, (2 * WINDOW, 3 * WINDOW), 1) % WINDOW
    mine_row = t * HEADS

    def attend(n, key_band, value_band, allowed):
        lanes = pl.ds(pl.multiple_of(n * WINDOW, WINDOW), WINDOW)
        q = jnp.concatenate([q_v[pl.ds(g * HEAD_SIZE, HEAD_SIZE), lanes] for g in range(3)], axis=1)
        scores = dot(key_band, q, ((0,), (0,))) * HEAD_SIZE**-0.5
        masked = jnp.where(allowed, scores, -1e30)
        top = jnp.maximum(jnp.max(masked, axis=0, keepdims=True), sinks)
        powers = jnp.where(allowed, jnp.exp(masked - top), 0.0)
        denom = jnp.sum(powers, axis=0, keepdims=True) + jnp.exp(sinks - top)
        probs = (powers * (1.0 / denom)).astype(BF16)
        output = dot(value_band, probs, ((1,), (0,))).astype(BF16)
        for g in range(3):
            rows = pl.ds(pl.multiple_of(mine_row + g * HEAD_SIZE, HEAD_SIZE), HEAD_SIZE)
            att_all[rows, lanes] = output[:, g * WINDOW : (g + 1) * WINDOW]

    near = (key_at > query_at) & (key_at <= query_at + WINDOW)
    for copy in locals_[1:5]:
        copy.wait()
    sinks = jnp.concatenate([jnp.full((1, WINDOW), sink[g], F32) for g in range(3)], axis=1)

    def attend_blocks(low, high):
        @pl.loop(low, high)
        def _(n):
            band = pl.ds(pl.multiple_of((n - 1) * WINDOW, WINDOW), 2 * WINDOW)
            attend(n, k_v[:, band], v_v[:, band], near)

    PART = ROWS // 2
    FIRST = (PART, 0)

    def att_rows(yy, cc, part, low=0, count=HEADS):
        row = (yy * 2 + cc) * HEADS + low
        return att_all.at[pl.ds(pl.multiple_of(row, 32), count), pl.ds(FIRST[part], PART)]

    def att_copy(part, index, ref, target):
        k = part * 7 + (0, 1, 2, 2, 3, 4, 5, 6)[index]
        return remote(ref, ref, att_send.at[0], att_recv.at[k], target)

    def att_arrived(part, index, ref):
        att_copy(part, index, ref, partner).wait_recv()

    def att_begin(part):
        for d, by in DIRS:
            start(att_copy(part, d, att_rows(y, c, part), y_next[by]))

    def att_pass(part):
        for d, by in DIRS:
            near_y = ring(y, -by)
            att_arrived(part, d, att_rows(near_y, c, part))
            start(att_copy(part, 2 + d, att_rows(near_y, c, part, d * HALF, HALF), y_next[by]))
            start(att_copy(part, 5 + d, att_rows(near_y, c, part), partner))

    def mix(yy, part, first):
        rows = pl.ds(pl.multiple_of(yy * 2 * HEADS, 2 * HEADS), 2 * HEADS)

        @pl.loop(0, PART // TILE)
        def _(i):
            tokens = pl.ds(pl.multiple_of(FIRST[part] + i * TILE, TILE), TILE)
            total = dot(att_all[rows, tokens], w_all[rows, :], ((0,), (0,)))
            mixed[tokens, :] = total if first else mixed[tokens, :] + total

    def mix_near(part):
        for d, by in DIRS:
            near_y = ring(y, -by)
            att_arrived(part, 5 + d, att_rows(near_y, 1 - c, part))
            if part == 0:
                arrived(w_rows(near_y, 0, 0, 2 * HEADS), w_recv.at[2 + d])
            mix(near_y, part, False)

    def mix_far(part):
        far = ring(y, 2)
        att_arrived(part, 2, att_rows(far, c, part))
        start(att_copy(part, 7, att_rows(far, c, part), partner))
        if part == 0:
            arrived(w_rows(far, 0, 0, 2 * HEADS), w_recv.at[4])
        att_arrived(part, 7, att_rows(far, 1 - c, part))
        mix(far, part, False)

    lanes_of = lambda cc: pl.ds(pl.multiple_of(cc * FEATURES, 128), FEATURES)

    def x_block(yy, cc, part, quarter=None):
        low, count = (0, PART) if quarter is None else (quarter * TILE, TILE)
        return x_all.at[pl.ds(pl.multiple_of(yy * ROWS + FIRST[part] + low, TILE), count), lanes_of(cc)]

    ones = jnp.ones((8, FEATURES), BF16)
    sq_rows = pl.ds(pl.multiple_of(t * 8, 8), 8)

    def make_x(part):
        gains = gain[...].astype(F32).reshape(1, FEATURES)

        @pl.loop(0, PART // TILE)
        def _(i):
            tokens = pl.ds(pl.multiple_of(FIRST[part] + i * TILE, TILE), TILE)
            here = (res_v[tokens, :].astype(F32) + mixed[tokens, :]).astype(BF16)
            stream[tokens, :] = here
            wide = here.astype(F32)
            rows = pl.ds(pl.multiple_of(y * ROWS + FIRST[part] + i * TILE, TILE), TILE)
            x_all[rows, lanes_of(c)] = (wide * gains).astype(BF16)
            sq = wide * wide
            high = sq.astype(BF16)
            low = (sq - high.astype(F32)).astype(BF16)
            squares[sq_rows, tokens] = dot(ones, high, ((1,), (1,))) + dot(ones, low, ((1,), (1,)))

    def x_copy(part, index, ref, target):
        k = part * 7 + (0, 0, 1, 1, 2, 2, 3, 4, 5, 6)[index]
        return remote(ref, ref, x_send.at[0], x_recv.at[k], target)

    def x_arrived(part, index, ref):
        x_copy(part, index, ref, partner).wait_recv()

    def x_begin(part, second):
        for d, by in DIRS:
            quarter = 1 - d if second else d
            start(x_copy(part, 2 * second + d, x_block(y, c, part, quarter), y_next[by]))

    def x_pass(part):
        x_arrived(part, 0, x_block(y, c, part))
        for d, by in DIRS:
            start(x_copy(part, 4 + d, x_block(ring(y, -by), c, part, d), y_next[by]))

    def x_near(part):
        x_arrived(part, 2, x_block(y, c, part))
        for d, by in DIRS:
            start(x_copy(part, 7 + d, x_block(ring(y, -by), c, part), partner))

    def x_far(part):
        x_arrived(part, 4, x_block(ring(y, 2), c, part))
        start(x_copy(part, 9, x_block(ring(y, 2), c, part), partner))

    def hide(yy, part, first=False, last=False):
        @pl.loop(0, PART // TILE)
        def _(i):
            tokens = pl.ds(pl.multiple_of(FIRST[part] + i * TILE, TILE), TILE)
            rows = pl.ds(pl.multiple_of(yy * ROWS + FIRST[part] + i * TILE, TILE), TILE)
            for n in range(3):
                cols = pl.ds(n * 512, 512)
                total = dot(x_all[rows, :], up_all[pl.ds(pl.multiple_of(yy * 768, 768), 768), cols], ((1,), (0,)))
                if not first:
                    total = total + hidden[tokens, cols]
                if last:
                    units = jnp.square(jnp.maximum(total, 0.0)).astype(BF16)
                    act_t[cols, tokens] = jnp.transpose(units)
                else:
                    hidden[tokens, cols] = total

    attend_blocks(4, 8)
    att_begin(0)
    start(att_copy(0, 4, att_rows(y, c, 0), partner))
    attend_blocks(1, 4)
    for copy in halo_copies:
        copy.wait_recv()
    first_key = jnp.where(s == 0, WINDOW, 0)
    attend(
        0,
        jnp.concatenate([halo_k[...], k_v[:, 0:WINDOW]], axis=1),
        jnp.concatenate([halo_v[...], v_v[:, 0:WINDOW]], axis=1),
        near & (key_at >= first_key),
    )
    start(att_copy(1, 4, att_rows(y, c, 1), partner))
    w_pass_on()
    up_gather.second()
    for copy in locals_[5:]:
        copy.wait()
    arrived(w_rows(y, 1 - c), w_recv.at[1])
    for part in (0, 1):
        att_arrived(part, 4, att_rows(y, 1 - c, part))
        mix(y, part, True)
    att_pass(0)
    att_begin(1)
    up_gather.forward(0)
    up_gather.third()
    mix_near(0)
    mix_far(0)
    make_x(0)
    x_begin(0, False)
    att_pass(1)
    x_begin(0, True)
    start(x_copy(0, 6, x_block(y, c, 0), partner))
    up_gather.forward(1)
    up_gather.fourth()
    mix_near(1)
    x_pass(0)
    mix_far(1)
    make_x(1)
    x_begin(1, False)
    x_begin(1, True)
    start(x_copy(1, 6, x_block(y, c, 1), partner))
    for k in range(1, 8):
        ref = squares.at[sq_rows]
        start(remote(ref, ref, sq_send.at[0], sq_recv.at[0], (s, (t + k) % 8)))
    x_near(0)
    up_gather.forward(2)
    x_far(0)
    up_gather.last(0)
    x_arrived(0, 6, x_block(y, 1 - c, 0))
    for d, by in DIRS:
        x_arrived(0, 7 + d, x_block(ring(y, -by), 1 - c, 0))
    x_arrived(0, 9, x_block(ring(y, 2), 1 - c, 0))
    hide(z, 0, first=True)
    up_gather.forward(3)
    down_gather.first()
    x_pass(1)
    up_gather.last(1)
    hide(ring(z, -1), 0)
    x_near(1)
    up_gather.last(2)
    up_gather.last(3)
    hide(ring(z, 1), 0)
    hide(ring(z, 2), 0, last=True)
    x_far(1)
    x_arrived(1, 6, x_block(y, 1 - c, 1))
    hide(y, 1, first=True)
    for d, by in DIRS:
        x_arrived(1, 7 + d, x_block(ring(y, -by), 1 - c, 1))
        hide(ring(y, -by), 1)
        if d == 0:
            down_gather.second()
    x_arrived(1, 9, x_block(ring(y, 2), 1 - c, 1))
    hide(ring(y, 2), 1, last=True)

    GROUPS = [[(half, 0, j) for j in range(3)] for half in (0, 1)]
    GROUPS.append([(half, 0, 3) for half in (0, 1)])
    for k in range(4):
        GROUPS.append([(half, i, ORDER[half][k]) for half in (0, 1) for i in (1, 2)])
        GROUPS.append([(half, 3, ORDER[half][k]) for half in (0, 1)])

    def lanes(part):
        return pl.ds(pl.multiple_of(part * PART, PART), PART)

    class Piece:
        def __init__(self, half, i, j):
            sec, prim = down_gather.at(half)
            sec, prim = ring(sec, STEPS[i]), ring(prim, STEPS[j])
            zz, xx = (sec, prim) if half == 0 else (prim, sec)
            self.row = (zz * 4 + xx) * SHARD + half * HALF
            self.half = half
            self.part = (xx % 2) * 2 + half
            self.mine = xx // 2 == c
            self.away = (y - zz + 4) % 4
            self.pair = zz * 4 + self.part

        def rows(self, low=0, count=HALF):
            return pl.ds(pl.multiple_of(self.row + low, 16), count)

        def paired_rows(self, low=0, count=HALF):
            return pl.ds(pl.multiple_of(self.pair * HALF + low, 16), count)

        def to_pair(self, part):
            k = self.pair * 2 + part
            return remote(
                partials.at[self.rows(), lanes(part)], paired.at[self.paired_rows(), lanes(part)],
                pair_send.at[0], pair_recv.at[k], partner,
            )

        def to_side(self, part):
            k = self.part * 2 + part
            return remote(
                partials.at[self.rows(), lanes(part)],
                chained.at[pl.ds(pl.multiple_of(self.part * HALF, 32), HALF), lanes(part)],
                side_send.at[0], side_recv.at[k], y_next[-1 if self.half == 0 else 1],
            )

        def to_owner(self, part):
            index = (self.away // 2) * 4 + self.part
            return remote(
                partials.at[self.rows(), lanes(part)],
                final.at[pl.ds(pl.multiple_of(index * HALF, 32), HALF), lanes(part)],
                owner_send.at[0], owner_recv.at[part], (s, ring(y, -self.away) * 2 + c),
            )

        def add(self, part, side):
            rows = self.rows()
            total = partials[rows, lanes(part)].astype(F32) + paired[self.paired_rows(), lanes(part)].astype(F32)
            if side:
                there = pl.ds(pl.multiple_of(self.part * HALF, 32), HALF)
                total = total + chained[there, lanes(part)].astype(F32)
            partials[rows, lanes(part)] = total.astype(BF16)

    groups = [[Piece(*facts) for facts in group] for group in GROUPS]

    def compute(group):
        @pl.loop(0, 2)
        def _(part):
            @pl.loop(0, PART // TILE)
            def _(i):
                tokens = pl.ds(pl.multiple_of(part * PART + i * TILE, TILE), TILE)
                weight = jnp.concatenate([down_all[p.rows(), :] for p in group], axis=0)
                total = dot(weight, act_t[:, tokens], ((1,), (0,))).astype(BF16)
                for k, p in enumerate(group):
                    partials[p.rows(), tokens] = total[k * HALF : (k + 1) * HALF]

            for p in group:
                @pl.when(jnp.logical_not(p.mine))
                def _():
                    p.to_pair(part).start()

    def combine(group):
        @pl.loop(0, 2)
        def _(part):
            for p in group:
                side = 1 if p.half == 0 else 3

                @pl.when(p.mine & (p.away != 0) & (p.away != side))
                def _():
                    p.to_pair(part).wait_recv()
                    p.add(part, False)

                    @pl.when(p.away == 2)
                    def _():
                        p.to_side(part).start()

                    @pl.when(p.away != 2)
                    def _():
                        p.to_owner(part).start()

    def relay(group):
        @pl.loop(0, 2)
        def _(part):
            for p in group:
                @pl.when(p.mine & (p.away == (1 if p.half == 0 else 3)))
                def _():
                    p.to_pair(part).wait_recv()
                    p.to_side(part).wait_recv()
                    p.add(part, True)
                    p.to_owner(part).start()

    compute(groups[0])
    compute(groups[1])
    combine(groups[0])
    down_gather.forward(0)
    compute(groups[3])
    combine(groups[1])
    down_gather.third()
    compute(groups[2])
    combine(groups[3])
    combine(groups[2])
    down_gather.forward(1)
    down_gather.fourth()
    compute(groups[5])
    relay(groups[0])
    relay(groups[1])
    down_gather.last(0)
    combine(groups[5])
    compute(groups[4])
    combine(groups[4])
    relay(groups[3])
    for copy in halo_copies:
        copy.wait_send()
    sent(w_pass, w_send.at[0])
    sent(w_all.at[pl.ds(0, 7 * HEADS)], w_send.at[1])
    sent(att_all.at[pl.ds(0, 7 * HEADS)], att_send.at[0])
    sent(x_all.at[pl.ds(0, 7 * PART)], x_send.at[0])
    sent(squares.at[pl.ds(0, 56)], sq_send.at[0])
    up_gather.sent()
    down_gather.forward(2)
    compute(groups[7])
    relay(groups[2])
    combine(groups[7])
    down_gather.last(1)
    compute(groups[6])
    combine(groups[6])
    relay(groups[5])
    relay(groups[4])
    down_gather.forward(3)
    compute(groups[9])
    combine(groups[9])
    relay(groups[7])
    down_gather.last(2)
    compute(groups[8])
    combine(groups[8])
    relay(groups[6])
    down_gather.last(3)
    compute(groups[10])
    combine(groups[10])
    relay(groups[9])
    relay(groups[8])
    relay(groups[10])
    down_gather.sent()
    sent(paired, pair_send.at[0])

    arrived(squares.at[pl.ds(0, 56)], sq_recv.at[0])
    own = [Piece(half, 0, 0) for half in (0, 1, 0, 1)]
    for part, p in enumerate(own):
        p.part = part
        p.half = part % 2
        p.row = (y * 4 + c * 2) * SHARD + part * HALF
        p.pair = y * 4 + part
    mine = pl.ds(pl.multiple_of((y * 4 + c * 2) * SHARD, FEATURES), FEATURES)
    beside = pl.ds(pl.multiple_of(y * FEATURES, FEATURES), FEATURES)

    @pl.loop(0, 2)
    def _(part):
        for p in own:
            p.to_pair(part).wait_recv()
        arrived(final.at[pl.ds(0, FEATURES)], owner_recv.at[part])

        @pl.loop(0, PART // 128)
        def _(i):
            tokens = pl.ds(pl.multiple_of(part * PART + i * 128, 128), 128)
            total = partials[mine, tokens].astype(F32) + paired[beside, tokens].astype(F32)
            for k in range(2):
                total = total + final[k * FEATURES : (k + 1) * FEATURES, tokens].astype(F32)
            norm = squares[0:1, tokens]
            for k in range(1, 8):
                norm = norm + squares[8 * k : 8 * k + 1, tokens]
            total = total * (1.0 / (norm * (1.0 / D) + EPSILON))
            result[tokens, :] = (stream[tokens, :].astype(F32) + jnp.transpose(total)).astype(BF16)

    sent(chained, side_send.at[0])
    sent(final, owner_send.at[0])


def body(
    queries, key_heads, projected_value_heads, sink_logit_table, out_weight,
    residual, norm_gain, up_weight, down_weight,
):
    hbm = pl.BlockSpec(memory_space=pl.ANY)
    dma = pltpu.SemaphoreType.DMA
    return pl.pallas_call(
        kernel,
        out_shape=pltpu.VMEM((ROWS, FEATURES), BF16),
        in_specs=[hbm] * 9,
        out_specs=pl.BlockSpec(memory_space=pltpu.VMEM),
        scratch_shapes=[
            pltpu.VMEM((D, HIDDEN), BF16),
            pltpu.VMEM((D, HIDDEN), BF16),
            pltpu.VMEM((4 * ROWS, 2 * FEATURES), BF16),
            pltpu.VMEM((8 * HEADS, ROWS), BF16),
            pltpu.VMEM((8 * HEADS, FEATURES), BF16),
            pltpu.VMEM((2, HALF, 2 * FEATURES), BF16),
            pltpu.VMEM((ROWS, HIDDEN), F32),
            pltpu.VMEM((HIDDEN, ROWS), BF16),
            pltpu.VMEM((ROWS, FEATURES), F32),
            pltpu.VMEM((ROWS, FEATURES), BF16),
            pltpu.VMEM((ROWS, FEATURES), BF16),
            pltpu.VMEM((HEADS, ROWS), BF16),
            pltpu.VMEM((HEAD_SIZE, ROWS), BF16),
            pltpu.VMEM((HEAD_SIZE, ROWS), BF16),
            pltpu.VMEM((HEAD_SIZE, WINDOW), BF16),
            pltpu.VMEM((HEAD_SIZE, WINDOW), BF16),
            pltpu.VMEM((D, ROWS), BF16),
            pltpu.VMEM((D // 2, ROWS), BF16),
            pltpu.VMEM((FEATURES, ROWS), BF16),
            pltpu.VMEM((2 * FEATURES, ROWS), BF16),
            pltpu.VMEM((64, ROWS), F32),
            pltpu.SMEM((3,), F32),
            pltpu.VMEM((FEATURES,), BF16),
            dma((9,)), dma((2,)), dma((5,)), dma((2,)), dma((2,)), dma((2,)), dma((20,)),
            dma((1,)), dma((14,)), dma((1,)), dma((14,)), dma((1,)), dma((1,)),
            dma((1,)), dma((32,)), dma((1,)), dma((8,)), dma((1,)), dma((2,)),
        ],
        compiler_params=pltpu.CompilerParams(
            collective_id=0, has_side_effects=True, vmem_limit_bytes=60 * 2**20
        ),
    )(
        queries.T, key_heads.T, projected_value_heads.T, sink_logit_table, out_weight,
        residual, norm_gain, up_weight, down_weight.T,
    )


def solution(mesh):
    return jax.shard_map(
        body,
        mesh=mesh,
        in_specs=(
            P("sp", "tp"), P("sp", "tp"), P("sp", "tp"), P("tp"), P("tp", None),
            P("sp", "tp"), P("tp"), P("sp", "tp"), P("tp", "sp"),
        ),
        out_specs=P("sp", "tp"),
        check_vma=False,
    )
```
